512 devices in a mesh: grp: 2 (over y), sp: 32 (over z, core), tp: 8 (over x).
Axes of the slice: x: 8, y: 2, z: 16, core: 2. Of those that a mesh axis runs over, the one named last changes fastest.
The devices are a block of a 8x8x16 slice.
Arguments:
- tokens: bfloat16 [16384, 4096], P(('grp', 'sp')), parts along dimension 0, may hold values from -6 to 6
- norm_gain: bfloat16 [2, 4096], replicated, may hold values from 0.099609375 to 1.8984375
- w_query: bfloat16 [2, 4096, 2048], P(None, 'sp', 'tp'), may hold values from -0.09375 to 0.09375
- w_key: bfloat16 [2, 4096, 2048], P(None, 'sp', 'tp'), may hold values from -0.09375 to 0.09375
- w_value: bfloat16 [2, 4096, 2048], P(None, 'sp', 'tp'), may hold values from -0.09375 to 0.09375
- w_out: bfloat16 [2, 2048, 4096], P(None, 'tp', 'sp'), may hold values from -0.125 to 0.125
- offset_bias: float32 [2, 16, 15, 31], P(None, 'tp'), may hold values from -4 to 300
Outputs:
- mixed: bfloat16 [16384, 4096], P(('grp', 'sp')), parts along dimension 0
The draws below stay inside these ranges and needn't reach their ends.
There are 2 independent parts, one for each index of `grp`. The reference program is written for one: setup_inputs(seed, part) draws one part's arguments, and reference() takes and returns one part's arrays. A program takes and returns all parts, laid end to end along the dimension named above; an argument that names none is the same for every part. Nothing has to cross between parts.
All inputs are finite; a program needn't handle non-finite values.
Results may differ from the reference program's by a relative error of at most 0.013.
Values may be sent and summed in bfloat16 or wider, within the bound.
A program may use at most 128 MiB of HBM per device.

```python
import jax
import jax.numpy as jnp
from jax import lax

D = 4096
HEADS = 16
HD = 128
GRID_W = 64
KR = 8
KC = 16
LAYERS = 2
ROWS_DEV = 4
TOKENS = 8192
N_SP = 32
N_TP = 8


def draw_offset_bias(key, part):
    shape = (LAYERS, HEADS, 2 * KR - 1, 2 * KC - 1)
    first_key, second_key = jax.random.split(jax.random.fold_in(key, 17))
    base = jnp.clip(jax.random.normal(first_key, shape, jnp.float32), -4.0, 4.0)
    return base


def steps_of(key, shape, shards, least, largest):
    factor_of, own = 1.0, jax.random.fold_in(key, 6)
    for position, parts in shards:
        heights = jnp.exp(jax.random.uniform(jax.random.fold_in(own, position), (parts,), jnp.float32, least / len(shards), largest / len(shards)))
        factor_of = factor_of * jnp.repeat(heights, shape[position] // parts).reshape([-1 if axis == position else 1 for axis in range(len(shape))])
    return factor_of


def scatter_about(own_key, dims, scale, most, pieces=(), kind=jnp.bfloat16):
    values = jax.random.normal(own_key, dims, jnp.float32) * scale
    if len(pieces) > 0:
        values = steps_of(own_key, dims, pieces, -0.22, 0.18) * values
    return jnp.clip(values, min=-most, max=most).astype(kind)


def setup_inputs(seed: int = 0, part: int = 0) -> dict:
    key_list = jax.random.split(jax.random.key(seed), 8)
    part_keys = jax.random.split(jax.random.fold_in(key_list[7], part), 8)
    tokens = scatter_about(part_keys[0], (TOKENS, D), 1.0, 6.0, ((0, 32),))
    norm_gain = jnp.clip(1.0 + 0.18 * jax.random.normal(key_list[1], (LAYERS, D), jnp.float32), 0.099609375, 1.8984375).astype(jnp.bfloat16)
    w_query = scatter_about(key_list[2], (LAYERS, D, HEADS * HD), D ** -0.5, 0.09375, ((1, 32), (2, 8)))
    w_key = scatter_about(key_list[3], (LAYERS, D, HEADS * HD), D ** -0.5, 0.09375, ((1, 32), (2, 8)))
    w_value = scatter_about(key_list[4], (LAYERS, D, HEADS * HD), D ** -0.5, 0.09375, ((1, 32), (2, 8)))
    w_out = scatter_about(key_list[5], (LAYERS, HEADS * HD, D), (HEADS * HD) ** -0.5, 0.125, ((1, 8), (2, 32)))
    offset_bias = draw_offset_bias(jax.random.fold_in(key_list[7], 71), part)
    return dict(tokens=tokens, norm_gain=norm_gain, w_query=w_query, w_key=w_key, w_value=w_value, w_out=w_out, offset_bias=offset_bias)


norm_eps = 1e-06

def rms_rows(values, gain):
    wide = values.astype(jnp.float32)
    scaled = wide * lax.rsqrt(lax.optimization_barrier(jnp.mean(wide * wide, axis=-1, keepdims=True)) + norm_eps)
    return (scaled * gain.astype(jnp.float32)).astype(jnp.bfloat16)

def reference(tokens, norm_gain, w_query, w_key, w_value, w_out, offset_bias):
    grid_rows = ROWS_DEV * N_SP
    group_width = HEADS // N_TP * HD
    scale = HD ** (-0.5)
    columns = jnp.arange(GRID_W, dtype=jnp.int32)
    col_first = jnp.clip(columns - KC // 2, 0, GRID_W - KC)
    col_inside = (columns[None, :] >= col_first[:, None]) & (columns[None, :] < col_first[:, None] + KC)
    col_offset = jnp.clip(columns[None, :] - columns[:, None], 1 - KC, KC - 1) + KC - 1
    row_first = jnp.clip(jnp.arange(grid_rows, dtype=jnp.int32) - KR // 2, 0, grid_rows - KR)
    residual = tokens
    for layer_index in range(LAYERS):
        normed = rms_rows(residual, norm_gain[layer_index])
        queries = jnp.dot(normed, w_query[layer_index], preferred_element_type=jnp.float32).astype(jnp.bfloat16)
        keys = jnp.dot(normed, w_key[layer_index], preferred_element_type=jnp.float32).astype(jnp.bfloat16)
        values = jnp.dot(normed, w_value[layer_index], preferred_element_type=jnp.float32).astype(jnp.bfloat16)
        queries = queries.reshape(grid_rows, GRID_W, HEADS, HD)
        keys = keys.reshape(grid_rows, GRID_W, HEADS, HD)
        values = values.reshape(grid_rows, GRID_W, HEADS, HD)
        col_bias = offset_bias[layer_index].astype(jnp.float32)[:, :, col_offset]

        def attend_row(packed, keys=keys, values=values, col_bias=col_bias):
            row_index, row_queries = packed
            row_begin = row_first[row_index].astype(jnp.int32)
            row_keys = lax.dynamic_slice_in_dim(keys, row_begin, KR, 0).astype(jnp.float32)
            row_values = lax.dynamic_slice_in_dim(values, row_begin, KR, 0).astype(jnp.float32)
            picked = row_begin + jnp.arange(KR, dtype=jnp.int32) - row_index + KR - 1
            bias = jnp.transpose(col_bias[:, picked], (0, 2, 1, 3))
            scores = jnp.einsum('qhd,jkhd->hqjk', row_queries.astype(jnp.float32), row_keys) * scale + bias
            scores = jnp.where(col_inside[None, :, None, :], scores, -jnp.inf)
            weights = jax.nn.softmax(scores.reshape(HEADS, GRID_W, KR * GRID_W), axis=-1).astype(jnp.bfloat16)
            weights = lax.optimization_barrier(weights)
            weights = weights.reshape(HEADS, GRID_W, KR, GRID_W).astype(jnp.float32)
            return jnp.einsum('hqjk,jkhd->qhd', weights, row_values).astype(jnp.bfloat16)
        attended = lax.map(attend_row, (jnp.arange(grid_rows, dtype=jnp.int32), queries))
        attended = attended.reshape(grid_rows * GRID_W, HEADS * HD)
        branch = jnp.zeros(residual.shape, jnp.float32)
        for group_index in range(N_TP):
            lower = group_index * group_width
            rounded = jnp.dot(attended[:, lower:lower + group_width], w_out[layer_index][lower:lower + group_width], preferred_element_type=jnp.float32).astype(jnp.bfloat16)
            branch = branch + lax.optimization_barrier(rounded).astype(jnp.float32)
        residual = (residual.astype(jnp.float32) + branch).astype(jnp.bfloat16)
    return residual
```

```python
import functools

import jax
import jax.numpy as jnp
from jax import lax
from jax.experimental import pallas as pl
from jax.experimental.pallas import tpu as pltpu
from jax.sharding import PartitionSpec as P

HD = 128
GRID_W = 64
KR = 8
KC = 16
LAYERS = 2
LANES = 128
MESH = pl.DeviceIdType.MESH
F32 = jnp.float32
BF16 = jnp.bfloat16

norm_eps = 1e-06


def reach(n, parity):
    plus = n // 2 if parity == 0 else n // 2 - 1
    return plus, n - 1 - plus


def nt_dot(a, b):
    return lax.dot_general(a, b, (((1,), (1,)), ((), ())), preferred_element_type=F32)


def wait_bytes(ref, sem):
    pltpu.make_async_copy(ref, ref, sem).wait()


def send(src, dst, send_sem, recv_sem, device):
    pltpu.make_async_remote_copy(
        src_ref=src,
        dst_ref=dst,
        send_sem=send_sem,
        recv_sem=recv_sem,
        device_id=device,
        device_id_type=MESH,
    ).start()


def layers_kernel(
    nsp,
    nx,
    tok,
    gain0,
    gain1,
    wq,
    wk,
    wv,
    wout,
    bias,
    out,
    w0,
    w1,
    wo,
    wt,
    xn,
    acc,
    res,
    qbuf,
    kv,
    att,
    xbuf,
    ybuf,
    ss,
    ring_recv,
    part_recv,
    halo_recv,
    att_recv,
    x_recv,
    a2a_recv,
    z_send,
    part_send,
    halo_send,
    att_send,
    x_send,
    a2a_send,
    out_sem,
):
    nz = nsp // 2
    hz, hx = nz // 2, nx // 2
    me_s, me_x = lax.axis_index("sp"), lax.axis_index("tp")
    me_z, me_c = me_s // 2, me_s % 2
    toks, depth = tok.shape
    part = LANES // nx
    wide = 2 * HD
    piece_w = depth // nx
    rows = toks // GRID_W
    half = toks // 2

    def ring_s(step):
        return lax.rem(me_s + 2 * step + 2 * nsp, nsp)

    def ring_x(step):
        return lax.rem(me_x + step + nx, nx)

    z_dev = ({"sp": ring_s(1)}, {"sp": ring_s(-1)})
    x_dev = ({"tp": ring_x(1)}, {"tp": ring_x(-1)})
    partner = {"sp": me_s + 1 - 2 * me_c}
    halo_dev = (
        {"sp": lax.rem(me_s + nsp - 1, nsp)},
        {"sp": lax.rem(me_s + 1, nsp)},
    )

    barrier = pltpu.get_barrier_semaphore()
    peers = [*z_dev, *halo_dev] + [{"tp": ring_x(d)} for d in range(1, nx)]
    for peer in peers:
        pl.semaphore_signal(barrier, inc=1, device_id=peer, device_id_type=MESH)
    pl.semaphore_wait(barrier, len(peers))

    mats = (wk, wv, wq)
    kinds = (0, 1, 2)
    OUT = 3
    parity = (0, 1, 0, 1)

    def chunk(layer, kind, s):
        if kind == OUT:
            return wo.at[layer, s]
        return w0.at[kind, s] if layer == 0 else w1.at[kind, :, s]

    def part_sem(layer, kind, hop):
        if kind == OUT:
            return part_recv.at[hz + 1 + layer]
        return part_recv.at[hop] if layer == 0 else part_recv.at[hz + 3]

    def ring_slot(layer, kind, side, hop):
        return ring_recv.at[layer, kind, side * hz + hop - 1]

    def ring_start(layer, kind):
        dst = chunk(layer, kind, me_s)
        src = dst if kind == OUT else mats[kind].at[layer]
        for side in (0, 1):
            if reach(nz, parity[kind])[side] >= 1:
                send(src, dst, z_send.at[side], ring_slot(layer, kind, side, 1), z_dev[side])
        send(src, dst, part_send.at[layer], part_sem(layer, kind, 0), partner)

    def ring_hop(layer, kind, hop):
        for side in (0, 1):
            last = reach(nz, parity[kind])[side]
            if isinstance(hop, int) and hop > last:
                continue
            src = chunk(layer, kind, ring_s(-hop if side == 0 else hop))
            wait_bytes(src, ring_slot(layer, kind, side, hop))

            def onward(src=src, side=side):
                send(src, src, z_send.at[side], ring_slot(layer, kind, side, hop + 1), z_dev[side])

            if isinstance(hop, int):
                if hop < last:
                    onward()
            else:
                pl.when(hop < last)(onward)
            send(src, src, part_send.at[layer], part_sem(layer, kind, hop), partner)

    pending = []

    def service(count):
        for _ in range(min(count, len(pending))):
            ring_hop(*pending.pop(0))

    for kind in kinds:
        ring_start(0, kind)

    eye = (
        lax.broadcasted_iota(jnp.int32, (LANES, LANES), 0)
        == lax.broadcasted_iota(jnp.int32, (LANES, LANES), 1)
    ).astype(BF16)
    for layer in range(LAYERS):
        turned = nt_dot(eye, wout[layer]).astype(BF16)
        wt[layer] = turned.reshape(nx, part, wide)
    own_lanes = pl.ds(pl.multiple_of(me_x * wide, wide), wide)
    for layer in range(LAYERS):
        for d in range(1, nx):
            to = ring_x(d)
            send(
                wt.at[layer, to],
                wo.at[layer, me_s, :, own_lanes],
                a2a_send,
                a2a_recv.at[layer],
                {"tp": to},
            )
        wo[layer, me_s, :, own_lanes] = wt[layer, me_x]
    for kind in kinds:
        w0[kind, me_s] = mats[kind][0]
        w1[kind, :, me_s] = mats[kind][1]

    block = 32

    def norm_rows(i, carry):
        at = pl.ds(pl.multiple_of(i * block, block), block)
        x = tok[at, :].astype(F32)
        scaled = x * lax.rsqrt(jnp.mean(x * x, axis=-1, keepdims=True) + norm_eps)
        xn[at, :] = (scaled * gain0[...].astype(F32)).astype(BF16)
        return carry

    lax.fori_loop(0, toks // block, norm_rows, 0)

    wait_bytes(wt.at[0, pl.ds(0, nx - 1)], a2a_recv.at[0])
    ring_start(0, OUT)

    def qkv_block(z, kind):
        x = xn[:, pl.ds(pl.multiple_of(z * 2 * LANES, 2 * LANES), 2 * LANES)]
        w = w0[kind, pl.ds(2 * z, 2)].reshape(2 * LANES, wide)
        return jnp.dot(x, w, preferred_element_type=F32)

    wait_bytes(w0.at[0, pl.ds(0, 3)], part_recv.at[0])
    for kind in kinds:
        acc[:, kind * wide : (kind + 1) * wide] = qkv_block(me_z, kind)

    def two_sides(hop):
        wait_bytes(w0.at[:, pl.ds(0, 2)], part_recv.at[hop])
        before = lax.rem(me_z - hop + nz, nz)
        after = lax.rem(me_z + hop, nz)
        for kind in kinds:
            acc[:, kind * wide : (kind + 1) * wide] += qkv_block(before, kind) + qkv_block(
                after, kind
            )

    def ring_step(hop, carry):
        for kind in (*kinds, OUT):
            ring_hop(0, kind, hop)

        @pl.when(hop > 1)
        def _():
            two_sides(hop - 1)

        return carry

    lax.fori_loop(1, hz, ring_step, 0)

    group = nx * LANES
    sel_row = lax.broadcasted_iota(jnp.int32, (group, LANES), 0)
    sel_col = lax.broadcasted_iota(jnp.int32, (group, LANES), 1)
    pick = (sel_col // part) * LANES + me_x * part + sel_col % part
    sel = (sel_row == pick).astype(BF16)
    for g in range(depth // group):
        picked = jnp.dot(tok[:, g * group : (g + 1) * group], sel, preferred_element_type=F32)
        res[:, g * LANES : (g + 1) * LANES] = picked.astype(BF16)

    for kind in kinds:
        ring_hop(0, kind, hz)
    if hz > 1:
        two_sides(hz - 1)
    for kind in kinds:
        ring_start(1, kind)
    wait_bytes(w0.at[0, pl.ds(0, 3)], part_recv.at[hz])
    far = lax.rem(me_z + hz, nz)

    def store_kind(layer, kind, value):
        if kind == 2:
            qbuf[...] = value.astype(BF16)
            return
        kv[layer, kind, toks : 2 * toks] = value.astype(BF16)
        src = kv.at[layer, kind, pl.ds(toks, toks)]
        for side in (0, 1):
            dst = kv.at[layer, kind, pl.ds(2 * toks if side == 0 else 0, toks)]
            send(src, dst, halo_send.at[layer], halo_recv.at[layer, kind, side], halo_dev[side])

    for kind in kinds:
        store_kind(0, kind, acc[:, kind * wide : (kind + 1) * wide] + qkv_block(far, kind))
    ring_hop(0, OUT, hz)
    pending += [(1, kind, hop) for hop in range(1, hz + 1) for kind in kinds]

    q_col = lax.broadcasted_iota(jnp.int32, (GRID_W, KR * GRID_W), 0)
    k_col = lax.broadcasted_iota(jnp.int32, (GRID_W, KR * GRID_W), 1) % GRID_W
    first_col = jnp.clip(q_col - KC // 2, 0, GRID_W - KC)
    inside = (k_col >= first_col) & (k_col < first_col + KC)
    grid_rows = rows * nsp

    def attend(layer, i, head):
        row = me_s * rows + i
        start = jnp.clip(row - KR // 2, 0, grid_rows - KR) - (me_s * rows - rows)
        keys_at = pl.ds(pl.multiple_of(start * GRID_W, GRID_W), KR * GRID_W)
        lanes = slice(head * HD, (head + 1) * HD)
        q = qbuf[i * GRID_W : (i + 1) * GRID_W, lanes]
        scores = nt_dot(q, kv[layer, 0, keys_at, lanes]) * (HD**-0.5)
        offset = start - rows - i + KR - 1
        pairs = []
        for p in range(KR // 2):
            line = bias[layer, head, pl.ds(offset + 2 * p, 1), :]
            spread = jnp.broadcast_to(line, (GRID_W, LANES))
            pairs.append(pltpu.roll(spread, 0, 1, stride=1, stride_axis=0))
        scores = scores + jnp.concatenate(pairs, axis=1)
        scores = jnp.where(inside, scores, -jnp.inf)
        e = jnp.exp(scores - jnp.max(scores, axis=-1, keepdims=True))
        weights = (e / jnp.sum(e, axis=-1, keepdims=True)).astype(BF16)
        values = kv[layer, 1, keys_at, lanes]
        mixed = jnp.dot(weights, values, preferred_element_type=F32)
        att[layer, me_x, i, :, lanes] = mixed.astype(BF16)

    def att_hop(layer, i, hop):
        for side in (0, 1):
            last = reach(nx, i % 2)[side]
            if hop > last:
                continue
            src = att.at[layer, ring_x(-hop if side == 0 else hop), i]
            if hop > 0:
                wait_bytes(src, att_recv.at[layer, i, side * hx + hop - 1])
            if hop < last:
                slot = att_recv.at[layer, i, side * hx + hop]
                send(src, src, att_send.at[layer, side], slot, x_dev[side])

    def attention(layer):
        for kind in (0, 1):
            for side in (0, 1):
                dst = kv.at[layer, kind, pl.ds(2 * toks if side == 0 else 0, toks)]
                wait_bytes(dst, halo_recv.at[layer, kind, side])
        for i in range(rows):
            for head in (0, 1):
                attend(layer, i, head)
            att_hop(layer, i, 0)
            if layer == 0:
                service(1)
        for hop in range(1, hx + 1):
            for i in range(rows):
                att_hop(layer, i, hop)
            if layer == 0:
                service(2)

    def x_hop(layer, h, hop):
        buf = xbuf if layer == 0 else ybuf
        for side in (0, 1):
            last = reach(nx, h)[side]
            if hop > last:
                continue
            owner = ring_x(-hop if side == 0 else hop)
            src = buf.at[owner, h]
            if hop > 0:
                wait_bytes(src, x_recv.at[layer, h, side * hx + hop - 1])
            if hop < last:
                slot = x_recv.at[layer, h, side * hx + hop]
                send(src, src, x_send.at[layer, side], slot, x_dev[side])
            if layer == 1 and (hop > 0 or side == 0):
                pltpu.make_async_copy(src, out.at[owner, h], out_sem).start()

    def project(layer):
        wait_bytes(wo.at[layer, pl.ds(0, nz)], part_recv.at[hz + 1 + layer])
        buf = xbuf if layer == 0 else ybuf
        for h in (0, 1):
            total = None
            for x in range(nx):
                a = att[layer, x, h * (rows // 2) : (h + 1) * (rows // 2)].reshape(half, wide)
                w = wo[layer, :, :, x * wide : (x + 1) * wide].reshape(piece_w, wide)
                term = nt_dot(a, w)
                total = term if total is None else total + term
            own = res[h * half : (h + 1) * half] if layer == 0 else xbuf[me_x, h]
            buf[me_x, h] = (own.astype(F32) + total).astype(BF16)
            x_hop(layer, h, 0)

    attention(0)
    project(0)

    acc[...] = jnp.zeros_like(acc)
    ss[...] = jnp.zeros_like(ss)

    def qkv_piece(owner, h):
        at = slice(h * half, (h + 1) * half)
        x = xbuf[owner, h].astype(F32)
        squares = x * x
        partial = ss[at]
        for g in range(piece_w // LANES):
            partial = partial + squares[:, g * LANES : (g + 1) * LANES]
        ss[at] = partial
        xg = (x * gain1[owner]).astype(BF16)
        for kind in kinds:
            w = w1[kind, owner].reshape(piece_w, wide)
            lanes = slice(kind * wide, (kind + 1) * wide)
            acc[at, lanes] += jnp.dot(xg, w, preferred_element_type=F32)

    def owners(hop):
        if hop == 0 or hop == hx:
            return [ring_x(hop)]
        return [ring_x(-hop), ring_x(hop)]

    early = hx // 2
    share = -(-len(pending) // max(2 * early, 1))
    for hop in range(1, early + 1):
        for h in (0, 1):
            x_hop(0, h, hop)
            service(share)
    service(len(pending))
    wait_bytes(wt.at[1, pl.ds(0, nx - 1)], a2a_recv.at[1])
    ring_start(1, OUT)
    pending += [(1, OUT, hop) for hop in range(1, hz + 1)]
    wait_bytes(w0.at[:, pl.ds(0, nz)], part_recv.at[hz + 3])
    for hop in range(0, early + 1):
        for owner in owners(hop):
            for h in (0, 1):
                qkv_piece(owner, h)
        service(1)
    for hop in range(early + 1, hx + 1):
        for h in (0, 1):
            x_hop(0, h, hop)
        service(1)
        for owner in owners(hop):
            for h in (0, 1):
                qkv_piece(owner, h)
    mean = jnp.sum(ss[...], axis=-1, keepdims=True) * (1.0 / depth)
    scale = lax.rsqrt(mean + norm_eps)
    for kind in kinds:
        store_kind(1, kind, acc[:, kind * wide : (kind + 1) * wide] * scale)
    service(len(pending))
    attention(1)
    project(1)
    for hop in range(1, hx + 1):
        for h in (0, 1):
            x_hop(1, h, hop)

    wait_bytes(ybuf, out_sem)
    chunks = 4 * hz - 2
    for side in (0, 1):
        wait_bytes(w0.at[pl.ds(0, 2), pl.ds(0, chunks)], z_send.at[side])
        for layer in range(LAYERS):
            wait_bytes(att.at[0, pl.ds(0, 2 * hx - 1), pl.ds(0, 2)], att_send.at[layer, side])
            wait_bytes(xbuf.at[pl.ds(0, 2 * hx - 1), 0], x_send.at[layer, side])
    for layer in range(LAYERS):
        wait_bytes(w0.at[pl.ds(0, 2)], part_send.at[layer])
        wait_bytes(kv.at[layer, :, pl.ds(0, 2 * toks)], halo_send.at[layer])
    wait_bytes(wt.at[:, pl.ds(0, nx - 1)], a2a_send)


def reorder_kernel(nx, y, o):
    part = LANES // nx
    tiles = [y[x].reshape(-1, LANES).astype(F32) for x in range(nx)]
    group = lax.broadcasted_iota(jnp.int32, tiles[0].shape, 1) // part
    bit = 1
    while bit < nx:
        low = (group & bit) == 0
        for x in range(nx):
            if x & bit == 0:
                a, b = tiles[x], tiles[x | bit]
                tiles[x] = jnp.where(low, a, pltpu.roll(b, bit * part, 1))
                tiles[x | bit] = jnp.where(low, pltpu.roll(a, LANES - bit * part, 1), b)
        bit *= 2
    for x in range(nx):
        o[:, x * LANES : (x + 1) * LANES] = tiles[x].astype(BF16)


def on_device(tokens, norm_gain, w_query, w_key, w_value, w_out, offset_bias):
    nsp, nx = lax.axis_size("sp"), lax.axis_size("tp")
    nz = nsp // 2
    hz, hx = nz // 2, nx // 2
    toks, depth = tokens.shape
    part = LANES // nx
    piece_w = depth // nx
    wide = 2 * HD
    rows = toks // GRID_W
    half = toks // 2

    def split(w):
        return w.reshape(LAYERS, nx, part, wide)

    gain0 = norm_gain[0].reshape(1, depth)
    gain1 = norm_gain[1].astype(F32).reshape(nsp, nx, part).swapaxes(0, 1).reshape(nx, 1, piece_w)
    table = jnp.pad(offset_bias, ((0, 0), (0, 0), (0, 2), (0, LANES - 2 * KC + 1)))
    lines = jnp.roll(table[:, :, : 2 * KR], 1 - KC, axis=3)
    lines = lines + jnp.roll(table[:, :, 1 : 2 * KR + 1], GRID_W + 1 - KC, axis=3)

    vmem = pl.BlockSpec(memory_space=pltpu.VMEM)
    dma = pltpu.SemaphoreType.DMA
    y = pl.pallas_call(
        functools.partial(layers_kernel, nsp, nx),
        out_shape=jax.ShapeDtypeStruct((nx, 2, half, piece_w), BF16),
        in_specs=[vmem] * 8,
        out_specs=pl.BlockSpec(memory_space=pl.ANY),
        scratch_shapes=[
            pltpu.VMEM((3, nsp, nx, part, wide), BF16),
            pltpu.VMEM((3, nx, nsp, part, wide), BF16),
            pltpu.VMEM((LAYERS, nsp, part, nx * wide), BF16),
            pltpu.VMEM((LAYERS, nx, part, wide), BF16),
            pltpu.VMEM((toks, depth), BF16),
            pltpu.VMEM((toks, 3 * wide), F32),
            pltpu.VMEM((toks, piece_w), BF16),
            pltpu.VMEM((toks, wide), BF16),
            pltpu.VMEM((LAYERS, 2, 3 * toks, wide), BF16),
            pltpu.VMEM((LAYERS, nx, rows, GRID_W, wide), BF16),
            pltpu.VMEM((nx, 2, half, piece_w), BF16),
            pltpu.VMEM((nx, 2, half, piece_w), BF16),
            pltpu.VMEM((toks, LANES), F32),
            dma((LAYERS, 4, 2 * hz)),
            dma((hz + 4,)),
            dma((LAYERS, 2, 2)),
            dma((LAYERS, rows, 2 * hx)),
            dma((LAYERS, 2, 2 * hx)),
            dma((LAYERS,)),
            dma((2,)),
            dma((LAYERS,)),
            dma((LAYERS,)),
            dma((LAYERS, 2)),
            dma((LAYERS, 2)),
            dma(()),
            dma(()),
        ],
        compiler_params=pltpu.CompilerParams(
            collective_id=0, has_side_effects=True, vmem_limit_bytes=60 * 1024 * 1024
        ),
    )(tokens, gain0, gain1, split(w_query), split(w_key), split(w_value), w_out, lines)
    return pl.pallas_call(
        functools.partial(reorder_kernel, nx),
        grid=(piece_w // LANES,),
        out_shape=jax.ShapeDtypeStruct((toks, depth), BF16),
        in_specs=[pl.BlockSpec((nx, 2, half, LANES), lambda g: (0, 0, 0, g))],
        out_specs=pl.BlockSpec((toks, nx * LANES), lambda g: (0, g)),
    )(y)


def solution(mesh):
    return jax.shard_map(
        on_device,
        mesh=mesh,
        in_specs=(
            P(("grp", "sp"), None),
            P(),
            P(None, "sp", "tp"),
            P(None, "sp", "tp"),
            P(None, "sp", "tp"),
            P(None, "tp", "sp"),
            P(None, "tp", None, None),
        ),
        out_specs=P(("grp", "sp"), None),
        check_vma=False,
    )
```

```python
import functools

import jax
import jax.numpy as jnp
from jax import lax
from jax.experimental import pallas as pl
from jax.experimental.pallas import tpu as pltpu
from jax.sharding import PartitionSpec as P

HD = 128
GRID_W = 64
KR = 8
KC = 16
LAYERS = 2
LANES = 128
MESH = pl.DeviceIdType.MESH
F32 = jnp.float32
BF16 = jnp.bfloat16

norm_eps = 1e-06


def reach(n, parity):
    plus = n // 2 if parity == 0 else n // 2 - 1
    return plus, n - 1 - plus


def nt_dot(a, b):
    return lax.dot_general(a, b, (((1,), (1,)), ((), ())), preferred_element_type=F32)


def wait_bytes(ref, sem):
    pltpu.make_async_copy(ref, ref, sem).wait()


def send(src, dst, send_sem, recv_sem, device):
    pltpu.make_async_remote_copy(
        src_ref=src,
        dst_ref=dst,
        send_sem=send_sem,
        recv_sem=recv_sem,
        device_id=device,
        device_id_type=MESH,
    ).start()


def exchange(tiles):
    tiles, n = list(tiles), len(tiles)
    part = LANES // n
    group = lax.broadcasted_iota(jnp.int32, tiles[0].shape, 1) // part
    bit = 1
    while bit < n:
        low = (group & bit) == 0
        for x in range(n):
            if x & bit == 0:
                a, b = tiles[x], tiles[x | bit]
                tiles[x] = jnp.where(low, a, pltpu.roll(b, bit * part, 1))
                tiles[x | bit] = jnp.where(low, pltpu.roll(a, LANES - bit * part, 1), b)
        bit *= 2
    return tiles


def layers_kernel(
    nsp,
    nx,
    tok_hbm,
    gain,
    wq,
    wk,
    wv,
    wout_hbm,
    bias,
    out,
    tok,
    wout,
    w0,
    w1,
    wo,
    wt,
    xn,
    acc,
    res,
    qbuf,
    kv,
    att,
    xbuf,
    ybuf,
    ss,
    gain1,
    padded,
    lines,
    load_sem,
    ring_recv,
    part_recv,
    halo_recv,
    att_recv,
    x_recv,
    a2a_recv,
    z_send,
    part_send,
    halo_send,
    att_send,
    x_send,
    a2a_send,
    out_sem,
):
    nz = nsp // 2
    hz, hx = nz // 2, nx // 2
    me_s, me_x = lax.axis_index("sp"), lax.axis_index("tp")
    me_z, me_c = me_s // 2, me_s % 2
    toks, depth = tok.shape
    part = LANES // nx
    wide = 2 * HD
    piece_w = depth // nx
    rows = toks // GRID_W
    half = toks // 2

    def ring_s(step):
        return lax.rem(me_s + 2 * step + 2 * nsp, nsp)

    def ring_x(step):
        return lax.rem(me_x + step + nx, nx)

    z_dev = ({"sp": ring_s(1)}, {"sp": ring_s(-1)})
    x_dev = ({"tp": ring_x(1)}, {"tp": ring_x(-1)})
    partner = {"sp": me_s + 1 - 2 * me_c}
    halo_dev = (
        {"sp": lax.rem(me_s + nsp - 1, nsp)},
        {"sp": lax.rem(me_s + 1, nsp)},
    )

    mats = (wk, wv, wq)
    kinds = (0, 1, 2)
    OUTS = (3, 4)
    HALVES = (5, 6, 7, 8)
    parity = (0, 1, 0, 1, 1, 0, 1, 0, 1)

    loads = [pltpu.make_async_copy(mats[k].at[0], w0.at[k, me_s], load_sem.at[k]) for k in kinds]
    loads += [
        pltpu.make_async_copy(mats[k].at[1], w1.at[k, :, me_s], load_sem.at[3 + k]) for k in kinds
    ]
    loads.append(pltpu.make_async_copy(wout_hbm, wout, load_sem.at[6]))
    loads.append(pltpu.make_async_copy(tok_hbm, tok, load_sem.at[7]))
    for load in loads:
        load.start()

    barrier = pltpu.get_barrier_semaphore()
    peers = [*z_dev, *halo_dev] + [{"tp": ring_x(d)} for d in range(1, nx)]
    for peer in peers:
        pl.semaphore_signal(barrier, inc=1, device_id=peer, device_id_type=MESH)
    pl.semaphore_wait(barrier, len(peers))

    def chunk(layer, kind, s):
        if kind in OUTS:
            lanes = nx * wide // 2
            return wo.at[layer, s, :, pl.ds((kind - OUTS[0]) * lanes, lanes)]
        if kind in HALVES:
            which, part_of = divmod(kind - HALVES[0], 2)
            return w1.at[1 + which, pl.ds(part_of * hx, hx), s]
        return w0.at[kind, s] if layer == 0 else w1.at[kind, :, s]

    def part_sem(layer, kind, hop):
        if kind in OUTS:
            return part_recv.at[hz + 1 + layer]
        return part_recv.at[hop] if layer == 0 else part_recv.at[hz + 3]

    def ring_slot(layer, kind, side, hop):
        return ring_recv.at[layer, kind, side * hz + hop - 1]

    def ring_start(layer, kind):
        dst = chunk(layer, kind, me_s)
        for side in (0, 1):
            if reach(nz, parity[kind])[side] >= 1:
                send(dst, dst, z_send.at[side], ring_slot(layer, kind, side, 1), z_dev[side])
        send(dst, dst, part_send.at[layer], part_sem(layer, kind, 0), partner)

    def ring_hop(layer, kind, hop):
        for side in (0, 1):
            last = reach(nz, parity[kind])[side]
            if isinstance(hop, int) and hop > last:
                continue
            src = chunk(layer, kind, ring_s(-hop if side == 0 else hop))
            wait_bytes(src, ring_slot(layer, kind, side, hop))

            def onward(src=src, side=side):
                send(src, src, z_send.at[side], ring_slot(layer, kind, side, hop + 1), z_dev[side])

            if isinstance(hop, int):
                if hop < last:
                    onward()
            else:
                pl.when(hop < last)(onward)
            send(src, src, part_send.at[layer], part_sem(layer, kind, hop), partner)

    def hops(*groups):
        return [(ring_hop, layer, kind, hop) for layer, kind, hop in groups if 1 <= hop <= hz]

    first = [hops((0, 3, h), (0, 4, h), (1, 0, h)) for h in range(1, hz + 1)]
    lag = max(hz // 2, 1)
    second = [
        hops(*[(1, kind, h) for kind in HALVES], (1, 3, h - lag), (1, 4, h - lag))
        for h in range(1, hz + lag + 1)
    ]
    second[lag - 1] += [(ring_start, 1, kind) for kind in OUTS]
    first[max(len(first) - 3, 0)] += [(ring_start, 1, kind) for kind in HALVES]

    def service(group, count):
        for _ in range(min(count, len(group))):
            for step, *what in group.pop(0):
                step(*what)

    for kind in kinds:
        loads[kind].wait()
        ring_start(0, kind)

    loads[6].wait()
    eye = (
        lax.broadcasted_iota(jnp.int32, (LANES, LANES), 0)
        == lax.broadcasted_iota(jnp.int32, (LANES, LANES), 1)
    ).astype(BF16)
    for layer in range(LAYERS):
        turned = nt_dot(eye, wout[layer]).astype(BF16)
        wt[layer] = turned.reshape(nx, part, wide)
    own_lanes = pl.ds(pl.multiple_of(me_x * wide, wide), wide)
    for layer in range(LAYERS):
        for d in range(1, nx):
            to = ring_x(d)
            send(
                wt.at[layer, to],
                wo.at[layer, me_s, :, own_lanes],
                a2a_send,
                a2a_recv.at[layer],
                {"tp": to},
            )
        wo[layer, me_s, :, own_lanes] = wt[layer, me_x]
    loads[7].wait()
    block = 32

    def norm_rows(i, carry):
        at = pl.ds(pl.multiple_of(i * block, block), block)
        x = tok[at, :].astype(F32)
        scaled = x * lax.rsqrt(jnp.mean(x * x, axis=-1, keepdims=True) + norm_eps)
        xn[at, :] = (scaled * gain[0:1].astype(F32)).astype(BF16)
        return carry

    lax.fori_loop(0, toks // block, norm_rows, 0)

    for x, tile in enumerate(
        exchange(
            [
                jnp.concatenate(
                    [
                        gain[1:2, (g * nx + t) * LANES : (g * nx + t + 1) * LANES].astype(F32)
                        for g in range(piece_w // LANES)
                    ],
                    axis=0,
                )
                for t in range(nx)
            ]
        )
    ):
        for g in range(piece_w // LANES):
            gain1[x, :, g * LANES : (g + 1) * LANES] = tile[g : g + 1]
    padded[...] = jnp.zeros_like(padded)
    padded[:, : 2 * KR - 1, :, : 2 * KC - 1] = bias[...]
    for layer in range(LAYERS):
        for head in (0, 1):
            here = pltpu.roll(padded[layer, : 2 * KR, head, :], LANES + 1 - KC, 1)
            after = pltpu.roll(padded[layer, 1 : 2 * KR + 1, head, :], GRID_W + 1 - KC, 1)
            lines[layer, head] = here + after

    def qkv_block(z, kind):
        x = xn[:, pl.ds(pl.multiple_of(z * 2 * LANES, 2 * LANES), 2 * LANES)]
        w = w0[kind, pl.ds(2 * z, 2)].reshape(2 * LANES, wide)
        return jnp.dot(x, w, preferred_element_type=F32)

    wait_bytes(w0.at[0, pl.ds(0, 3)], part_recv.at[0])
    for kind in kinds:
        acc[:, kind * wide : (kind + 1) * wide] = qkv_block(me_z, kind)

    def two_sides(hop):
        wait_bytes(w0.at[:, pl.ds(0, 2)], part_recv.at[hop])
        before = lax.rem(me_z - hop + nz, nz)
        after = lax.rem(me_z + hop, nz)
        for kind in kinds:
            acc[:, kind * wide : (kind + 1) * wide] += qkv_block(before, kind) + qkv_block(
                after, kind
            )

    def ring_step(hop, carry):
        for kind in kinds:
            ring_hop(0, kind, hop)

        @pl.when(hop > 1)
        def _():
            two_sides(hop - 1)

        return carry

    lax.fori_loop(1, hz, ring_step, 0)

    group = nx * LANES
    sel_row = lax.broadcasted_iota(jnp.int32, (group, LANES), 0)
    sel_col = lax.broadcasted_iota(jnp.int32, (group, LANES), 1)
    pick = (sel_col // part) * LANES + me_x * part + sel_col % part
    sel = (sel_row == pick).astype(BF16)
    for g in range(depth // group):
        picked = jnp.dot(tok[:, g * group : (g + 1) * group], sel, preferred_element_type=F32)
        res[:, g * LANES : (g + 1) * LANES] = picked.astype(BF16)

    for kind in kinds:
        ring_hop(0, kind, hz)
    if hz > 1:
        two_sides(hz - 1)
    wait_bytes(w0.at[0, pl.ds(0, 3)], part_recv.at[hz])
    far = lax.rem(me_z + hz, nz)

    def store_kind(layer, kind, value):
        if kind == 2:
            qbuf[...] = value.astype(BF16)
            return
        kv[layer, kind, toks : 2 * toks] = value.astype(BF16)
        src = kv.at[layer, kind, pl.ds(toks, toks)]
        for side in (0, 1):
            dst = kv.at[layer, kind, pl.ds(2 * toks if side == 0 else 0, toks)]
            send(src, dst, halo_send.at[layer], halo_recv.at[layer, kind, side], halo_dev[side])

    for kind in kinds:
        store_kind(0, kind, acc[:, kind * wide : (kind + 1) * wide] + qkv_block(far, kind))
    for layer in range(LAYERS):
        wait_bytes(wt.at[layer, pl.ds(0, nx - 1)], a2a_recv.at[layer])
    for kind in kinds:
        loads[3 + kind].wait()
    for kind in OUTS:
        ring_start(0, kind)
    ring_start(1, 0)

    q_col = lax.broadcasted_iota(jnp.int32, (GRID_W, KR * GRID_W), 0)
    k_col = lax.broadcasted_iota(jnp.int32, (GRID_W, KR * GRID_W), 1) % GRID_W
    first_col = jnp.clip(q_col - KC // 2, 0, GRID_W - KC)
    inside = (k_col >= first_col) & (k_col < first_col + KC)
    grid_rows = rows * nsp

    def span(i):
        start = jnp.clip(me_s * rows + i - KR // 2, 0, grid_rows - KR) - (me_s * rows - rows)
        return start, pl.ds(pl.multiple_of(start * GRID_W, GRID_W), KR * GRID_W)

    def weigh(layer, i, head):
        start, keys_at = span(i)
        lanes = slice(head * HD, (head + 1) * HD)
        q = qbuf[i * GRID_W : (i + 1) * GRID_W, lanes]
        scores = nt_dot(q, kv[layer, 0, keys_at, lanes]) * (HD**-0.5)
        offset = start - rows - i + KR - 1
        pairs = []
        for p in range(KR // 2):
            line = lines[layer, head, pl.ds(offset + 2 * p, 1), :]
            spread = jnp.broadcast_to(line, (GRID_W, LANES))
            pairs.append(pltpu.roll(spread, 0, 1, stride=1, stride_axis=0))
        scores = scores + jnp.concatenate(pairs, axis=1)
        scores = jnp.where(inside, scores, -jnp.inf)
        e = jnp.exp(scores - jnp.max(scores, axis=-1, keepdims=True))
        return (e / jnp.sum(e, axis=-1, keepdims=True)).astype(BF16)

    def mix(layer, i, head, weights):
        lanes = slice(head * HD, (head + 1) * HD)
        values = kv[layer, 1, span(i)[1], lanes]
        mixed = jnp.dot(weights, values, preferred_element_type=F32)
        att[layer, me_x, i, :, lanes] = mixed.astype(BF16)

    def att_hop(layer, i, hop):
        for side in (0, 1):
            last = reach(nx, i % 2)[side]
            if hop > last:
                continue
            src = att.at[layer, ring_x(-hop if side == 0 else hop), i]
            if hop > 0:
                wait_bytes(src, att_recv.at[layer, i, side * hx + hop - 1])
            if hop < last:
                slot = att_recv.at[layer, i, side * hx + hop]
                send(src, src, att_send.at[layer, side], slot, x_dev[side])

    def halo_wait(layer, kind):
        for side in (0, 1):
            dst = kv.at[layer, kind, pl.ds(2 * toks if side == 0 else 0, toks)]
            wait_bytes(dst, halo_recv.at[layer, kind, side])

    def attention(layer, group, counts):
        halo_wait(layer, 0)
        for i in range(0, rows, 2):
            weights = [weigh(layer, i + n // 2, n % 2) for n in range(4)]
            if i == 0:
                halo_wait(layer, 1)
            for n in range(4):
                mix(layer, i + n // 2, n % 2, weights[n])
            att_hop(layer, i, 0)
            att_hop(layer, i + 1, 0)
            service(group, counts[i // 2])
        for hop in range(1, hx + 1):
            for i in range(rows):
                att_hop(layer, i, hop)
            service(group, counts[1 + hop] if 1 + hop < len(counts) else 1)
        service(group, len(group))

    def x_hop(layer, h, hop):
        buf = xbuf if layer == 0 else ybuf
        for side in (0, 1):
            last = reach(nx, h)[side]
            if hop > last:
                continue
            owner = ring_x(-hop if side == 0 else hop)
            src = buf.at[owner, h]
            if hop > 0:
                wait_bytes(src, x_recv.at[layer, h, side * hx + hop - 1])
            if hop < last:
                slot = x_recv.at[layer, h, side * hx + hop]
                send(src, src, x_send.at[layer, side], slot, x_dev[side])
            if layer == 1 and (hop > 0 or side == 0):
                pltpu.make_async_copy(src, out.at[owner, h], out_sem).start()

    def project(layer):
        wait_bytes(wo.at[layer, pl.ds(0, nz)], part_recv.at[hz + 1 + layer])
        buf = xbuf if layer == 0 else ybuf
        for h in (0, 1):
            total = None
            for x in range(nx):
                a = att[layer, x, h * (rows // 2) : (h + 1) * (rows // 2)].reshape(half, wide)
                w = wo[layer, :, :, x * wide : (x + 1) * wide].reshape(piece_w, wide)
                term = nt_dot(a, w)
                total = term if total is None else total + term
            own = res[h * half : (h + 1) * half] if layer == 0 else xbuf[me_x, h]
            buf[me_x, h] = (own.astype(F32) + total).astype(BF16)
            x_hop(layer, h, 0)

    attention(0, first, (1, 1, 1, 2, 2, 1))
    project(0)

    ss[...] = jnp.zeros_like(ss)

    def take_piece(owner, h):
        def some_rows(i, carry):
            at = pl.ds(pl.multiple_of(i * block, block), block)
            to = pl.ds(pl.multiple_of(h * half + i * block, block), block)
            x = xbuf[owner, h, at].astype(F32)
            squares = x * x
            total = ss[to]
            for g in range(piece_w // LANES):
                total = total + squares[:, g * LANES : (g + 1) * LANES]
            ss[to] = total
            lanes = pl.ds(pl.multiple_of(owner * piece_w, piece_w), piece_w)
            xn[to, lanes] = (x * gain1[owner]).astype(BF16)
            return carry

        lax.fori_loop(0, half // block, some_rows, 0)

    share = -(-hz // hx)
    for h in (0, 1):
        take_piece(me_x, h)
    for hop in range(1, hx + 1):
        for h in (0, 1):
            x_hop(0, h, hop)
            if h == 1:
                service(second, share)
            for owner in {0: [ring_x(-hop)], 1: [ring_x(hop)]}[h] if hop == hx else [
                ring_x(-hop),
                ring_x(hop),
            ]:
                take_piece(owner, h)
    service(second, len(second) - lag)
    wait_bytes(w0.at[:, pl.ds(0, nz)], part_recv.at[hz + 3])
    mean = jnp.sum(ss[...], axis=-1, keepdims=True) * (1.0 / depth)
    scale = lax.rsqrt(mean + norm_eps)
    for kind in kinds:
        w = w1[kind].reshape(depth, wide)
        store_kind(1, kind, jnp.dot(xn[...], w, preferred_element_type=F32) * scale)
    attention(1, second, (1, 1, 1, 1, 1, 1))
    project(1)
    for hop in range(1, hx + 1):
        for h in (0, 1):
            x_hop(1, h, hop)

    wait_bytes(ybuf, out_sem)
    chunks = 4 * hz - 2
    for side in (0, 1):
        wait_bytes(w0.at[pl.ds(0, 2), pl.ds(0, chunks)], z_send.at[side])
        for layer in range(LAYERS):
            wait_bytes(att.at[0, pl.ds(0, 2 * hx - 1), pl.ds(0, 2)], att_send.at[layer, side])
            wait_bytes(xbuf.at[pl.ds(0, 2 * hx - 1), 0], x_send.at[layer, side])
    for layer in range(LAYERS):
        wait_bytes(w0.at[pl.ds(0, 2)], part_send.at[layer])
        wait_bytes(kv.at[layer, :, pl.ds(0, 2 * toks)], halo_send.at[layer])
    wait_bytes(wt.at[:, pl.ds(0, nx - 1)], a2a_send)


def reorder_kernel(nx, y, o):
    half = y.shape[2]
    block = 32

    def some_rows(i, carry):
        at = pl.ds(pl.multiple_of(i * block, block), block)
        for h in (0, 1):
            to = pl.ds(pl.multiple_of(h * half + i * block, block), block)
            tiles = exchange([y[x, h, at, :].astype(F32) for x in range(nx)])
            for x in range(nx):
                o[to, x * LANES : (x + 1) * LANES] = tiles[x].astype(BF16)
        return carry

    lax.fori_loop(0, half // block, some_rows, 0)


def on_device(tokens, norm_gain, w_query, w_key, w_value, w_out, offset_bias):
    nsp, nx = lax.axis_size("sp"), lax.axis_size("tp")
    nz = nsp // 2
    hz, hx = nz // 2, nx // 2
    toks, depth = tokens.shape
    part = LANES // nx
    piece_w = depth // nx
    wide = 2 * HD
    rows = toks // GRID_W
    half = toks // 2

    def split(w):
        return w.reshape(LAYERS, nx, part, wide)

    vmem = pl.BlockSpec(memory_space=pltpu.VMEM)
    hbm = pl.BlockSpec(memory_space=pl.ANY)
    dma = pltpu.SemaphoreType.DMA
    y = pl.pallas_call(
        functools.partial(layers_kernel, nsp, nx),
        out_shape=jax.ShapeDtypeStruct((nx, 2, half, piece_w), BF16),
        in_specs=[hbm, vmem, hbm, hbm, hbm, hbm, vmem],
        out_specs=hbm,
        scratch_shapes=[
            pltpu.VMEM((toks, depth), BF16),
            pltpu.VMEM((LAYERS, wide, LANES), BF16),
            pltpu.VMEM((3, nsp, nx, part, wide), BF16),
            pltpu.VMEM((3, nx, nsp, part, wide), BF16),
            pltpu.VMEM((LAYERS, nsp, part, nx * wide), BF16),
            pltpu.VMEM((LAYERS, nx, part, wide), BF16),
            pltpu.VMEM((toks, depth), BF16),
            pltpu.VMEM((toks, 3 * wide), F32),
            pltpu.VMEM((toks, piece_w), BF16),
            pltpu.VMEM((toks, wide), BF16),
            pltpu.VMEM((LAYERS, 2, 3 * toks, wide), BF16),
            pltpu.VMEM((LAYERS, nx, rows, GRID_W, wide), BF16),
            pltpu.VMEM((nx, 2, half, piece_w), BF16),
            pltpu.VMEM((nx, 2, half, piece_w), BF16),
            pltpu.VMEM((toks, LANES), F32),
            pltpu.VMEM((nx, 1, piece_w), F32),
            pltpu.VMEM((LAYERS, 2 * KR + 1, 2, LANES), F32),
            pltpu.VMEM((LAYERS, 2, 2 * KR, LANES), F32),
            dma((8,)),
            dma((LAYERS, 9, 2 * hz)),
            dma((hz + 4,)),
            dma((LAYERS, 2, 2)),
            dma((LAYERS, rows, 2 * hx)),
            dma((LAYERS, 2, 2 * hx)),
            dma((LAYERS,)),
            dma((2,)),
            dma((LAYERS,)),
            dma((LAYERS,)),
            dma((LAYERS, 2)),
            dma((LAYERS, 2)),
            dma(()),
            dma(()),
        ],
        compiler_params=pltpu.CompilerParams(
            collective_id=0, has_side_effects=True, vmem_limit_bytes=60 * 1024 * 1024
        ),
    )(
        tokens,
        norm_gain,
        split(w_query),
        split(w_key),
        split(w_value),
        w_out,
        offset_bias.swapaxes(1, 2),
    )
    return pl.pallas_call(
        functools.partial(reorder_kernel, nx),
        grid=(piece_w // LANES,),
        out_shape=jax.ShapeDtypeStruct((toks, depth), BF16),
        in_specs=[pl.BlockSpec((nx, 2, half, LANES), lambda g: (0, 0, 0, g))],
        out_specs=pl.BlockSpec((toks, nx * LANES), lambda g: (0, g)),
    )(y)


def solution(mesh):
    return jax.shard_map(
        on_device,
        mesh=mesh,
        in_specs=(
            P(("grp", "sp"), None),
            P(),
            P(None, "sp", "tp"),
            P(None, "sp", "tp"),
            P(None, "sp", "tp"),
            P(None, "tp", "sp"),
            P(None, "tp", None, None),
        ),
        out_specs=P(("grp", "sp"), None),
        check_vma=False,
    )
```

```python
import functools

import jax
import jax.numpy as jnp
from jax import lax
from jax.experimental import pallas as pl
from jax.experimental.pallas import tpu as pltpu
from jax.sharding import PartitionSpec as P

HD = 128
GRID_W = 64
KR = 8
KC = 16
LAYERS = 2
LANES = 128
MESH = pl.DeviceIdType.MESH
F32 = jnp.float32
BF16 = jnp.bfloat16

norm_eps = 1e-06


def reach(n, parity):
    plus = n // 2 if parity == 0 else n // 2 - 1
    return plus, n - 1 - plus


def nt_dot(a, b):
    return lax.dot_general(a, b, (((1,), (1,)), ((), ())), preferred_element_type=F32)


def wait_bytes(ref, sem):
    pltpu.make_async_copy(ref, ref, sem).wait()


def send(src, dst, send_sem, recv_sem, device):
    pltpu.make_async_remote_copy(
        src_ref=src,
        dst_ref=dst,
        send_sem=send_sem,
        recv_sem=recv_sem,
        device_id=device,
        device_id_type=MESH,
    ).start()


def exchange(tiles):
    tiles, n = list(tiles), len(tiles)
    part = LANES // n
    group = lax.broadcasted_iota(jnp.int32, tiles[0].shape, 1) // part
    bit = 1
    while bit < n:
        low = (group & bit) == 0
        for x in range(n):
            if x & bit == 0:
                a, b = tiles[x], tiles[x | bit]
                tiles[x] = jnp.where(low, a, pltpu.roll(b, bit * part, 1))
                tiles[x | bit] = jnp.where(low, pltpu.roll(a, LANES - bit * part, 1), b)
        bit *= 2
    return tiles


def layers_kernel(
    nsp,
    nx,
    tok_hbm,
    gain,
    wq,
    wk,
    wv,
    wout_hbm,
    bias,
    out,
    tok,
    wout,
    w0,
    w1,
    wo,
    wt,
    xn,
    acc,
    res,
    qbuf,
    kv,
    att,
    xbuf,
    ybuf,
    ss,
    gain1,
    padded,
    lines,
    load_sem,
    ring_recv,
    part_recv,
    halo_recv,
    att_recv,
    x_recv,
    a2a_recv,
    z_send,
    part_send,
    halo_send,
    att_send,
    x_send,
    a2a_send,
    out_sem,
):
    nz = nsp // 2
    hz, hx = nz // 2, nx // 2
    me_s, me_x = lax.axis_index("sp"), lax.axis_index("tp")
    me_z, me_c = me_s // 2, me_s % 2
    toks, depth = tok.shape
    part = LANES // nx
    wide = 2 * HD
    piece_w = depth // nx
    rows = toks // GRID_W
    half = toks // 2

    def ring_s(step):
        return lax.rem(me_s + 2 * step + 2 * nsp, nsp)

    def ring_x(step):
        return lax.rem(me_x + step + nx, nx)

    z_dev = ({"sp": ring_s(1)}, {"sp": ring_s(-1)})
    x_dev = ({"tp": ring_x(1)}, {"tp": ring_x(-1)})
    partner = {"sp": me_s + 1 - 2 * me_c}
    halo_dev = (
        {"sp": lax.rem(me_s + nsp - 1, nsp)},
        {"sp": lax.rem(me_s + 1, nsp)},
    )

    mats = (wk, wv, wq)
    kinds = (0, 1, 2)
    OUT = 3
    parity = (0, 1, 0, 1)
    lag = max(hz // 2, 1)

    loads = [pltpu.make_async_copy(mats[k].at[0], w0.at[k, me_s], load_sem.at[k]) for k in kinds]
    loads += [
        pltpu.make_async_copy(mats[k].at[1], w1.at[k, :, me_s], load_sem.at[3 + k]) for k in kinds
    ]
    loads.append(pltpu.make_async_copy(wout_hbm, wout, load_sem.at[6]))
    loads.append(pltpu.make_async_copy(tok_hbm, tok, load_sem.at[7]))
    for load in loads:
        load.start()

    barrier = pltpu.get_barrier_semaphore()
    peers = [*z_dev, *halo_dev] + [{"tp": ring_x(d)} for d in range(1, nx)]
    for peer in peers:
        pl.semaphore_signal(barrier, inc=1, device_id=peer, device_id_type=MESH)
    pl.semaphore_wait(barrier, len(peers))

    def chunk(layer, kind, s):
        if kind == OUT:
            return wo.at[layer, s]
        return w0.at[kind, s] if layer == 0 else w1.at[kind, :, s]

    def part_sem(layer, kind, hop):
        if kind == OUT:
            return part_recv.at[hz + 1 + layer]
        if layer == 1:
            return part_recv.at[hz + 3]
        if isinstance(hop, int) and hop == hz:
            return part_recv.at[(hz, hz + 4, hz + 5)[kind]]
        return part_recv.at[hop]

    def ring_slot(layer, kind, side, hop):
        return ring_recv.at[layer, kind, side * hz + hop - 1]

    def ring_start(layer, kind):
        dst = chunk(layer, kind, me_s)
        for side in (0, 1):
            if reach(nz, parity[kind])[side] >= 1:
                send(dst, dst, z_send.at[side], ring_slot(layer, kind, side, 1), z_dev[side])
        send(dst, dst, part_send.at[layer], part_sem(layer, kind, 0), partner)

    def ring_hop(layer, kind, hop):
        for side in (0, 1):
            last = reach(nz, parity[kind])[side]
            if isinstance(hop, int) and hop > last:
                continue
            src = chunk(layer, kind, ring_s(-hop if side == 0 else hop))
            wait_bytes(src, ring_slot(layer, kind, side, hop))

            def onward(src=src, side=side):
                send(src, src, z_send.at[side], ring_slot(layer, kind, side, hop + 1), z_dev[side])

            if isinstance(hop, int):
                if hop < last:
                    onward()
            else:
                pl.when(hop < last)(onward)
            send(src, src, part_send.at[layer], part_sem(layer, kind, hop), partner)

    offsets = {(0, OUT): lag, (1, 0): hz, (1, 1): hz, (1, 2): hz + lag, (1, OUT): hz + 2 * lag}

    def run_slot(slot):
        for what, offset in offsets.items():
            if 1 <= slot - offset <= hz:
                ring_hop(*what, slot - offset)
        for what, offset in offsets.items():
            if slot == offset:
                ring_start(*what)

    slots = list(range(hz + 1, 2 * hz + 2 * lag + 1))

    def service(count, until=None):
        for _ in range(min(count, len(slots))):
            if until is None or slots[0] <= until:
                run_slot(slots.pop(0))

    for kind in kinds:
        loads[kind].wait()
        ring_start(0, kind)

    loads[6].wait()
    eye = (
        lax.broadcasted_iota(jnp.int32, (LANES, LANES), 0)
        == lax.broadcasted_iota(jnp.int32, (LANES, LANES), 1)
    ).astype(BF16)
    for layer in range(LAYERS):
        turned = nt_dot(eye, wout[layer]).astype(BF16)
        wt[layer] = turned.reshape(nx, part, wide)
    own_lanes = pl.ds(pl.multiple_of(me_x * wide, wide), wide)
    for layer in range(LAYERS):
        for d in range(1, nx):
            to = ring_x(d)
            send(
                wt.at[layer, to],
                wo.at[layer, me_s, :, own_lanes],
                a2a_send,
                a2a_recv.at[layer],
                {"tp": to},
            )
        wo[layer, me_s, :, own_lanes] = wt[layer, me_x]
    loads[7].wait()
    block = 32

    def norm_rows(i, carry):
        at = pl.ds(pl.multiple_of(i * block, block), block)
        x = tok[at, :].astype(F32)
        scaled = x * lax.rsqrt(jnp.mean(x * x, axis=-1, keepdims=True) + norm_eps)
        xn[at, :] = (scaled * gain[0:1].astype(F32)).astype(BF16)
        return carry

    lax.fori_loop(0, toks // block, norm_rows, 0)

    for x, tile in enumerate(
        exchange(
            [
                jnp.concatenate(
                    [
                        gain[1:2, (g * nx + t) * LANES : (g * nx + t + 1) * LANES].astype(F32)
                        for g in range(piece_w // LANES)
                    ],
                    axis=0,
                )
                for t in range(nx)
            ]
        )
    ):
        for g in range(piece_w // LANES):
            gain1[x, :, g * LANES : (g + 1) * LANES] = tile[g : g + 1]
    padded[...] = jnp.zeros_like(padded)
    padded[:, : 2 * KR - 1, :, : 2 * KC - 1] = bias[...]
    for layer in range(LAYERS):
        for head in (0, 1):
            here = pltpu.roll(padded[layer, : 2 * KR, head, :], LANES + 1 - KC, 1)
            after = pltpu.roll(padded[layer, 1 : 2 * KR + 1, head, :], GRID_W + 1 - KC, 1)
            lines[layer, head] = here + after

    def qkv_block(z, kind):
        x = xn[:, pl.ds(pl.multiple_of(z * 2 * LANES, 2 * LANES), 2 * LANES)]
        w = w0[kind, pl.ds(2 * z, 2)].reshape(2 * LANES, wide)
        return jnp.dot(x, w, preferred_element_type=F32)

    wait_bytes(w0.at[0, pl.ds(0, 3)], part_recv.at[0])
    for kind in kinds:
        acc[:, kind * wide : (kind + 1) * wide] = qkv_block(me_z, kind)

    def two_sides(hop):
        wait_bytes(w0.at[:, pl.ds(0, 2)], part_recv.at[hop])
        before = lax.rem(me_z - hop + nz, nz)
        after = lax.rem(me_z + hop, nz)
        for kind in kinds:
            acc[:, kind * wide : (kind + 1) * wide] += qkv_block(before, kind) + qkv_block(
                after, kind
            )

    def ring_step(with_out, hop, carry):
        for kind in kinds:
            ring_hop(0, kind, hop)
        if with_out:
            ring_hop(0, OUT, hop - lag)

        @pl.when(hop > 1)
        def _():
            two_sides(hop - 1)

        return carry

    split_at = min(lag + 1, hz)
    lax.fori_loop(1, split_at, functools.partial(ring_step, False), 0)
    for layer in range(LAYERS):
        wait_bytes(wt.at[layer, pl.ds(0, nx - 1)], a2a_recv.at[layer])
    if lag < hz:
        ring_start(0, OUT)
    lax.fori_loop(split_at, hz, functools.partial(ring_step, True), 0)

    group = nx * LANES
    sel_row = lax.broadcasted_iota(jnp.int32, (group, LANES), 0)
    sel_col = lax.broadcasted_iota(jnp.int32, (group, LANES), 1)
    pick = (sel_col // part) * LANES + me_x * part + sel_col % part
    sel = (sel_row == pick).astype(BF16)
    for g in range(depth // group):
        picked = jnp.dot(tok[:, g * group : (g + 1) * group], sel, preferred_element_type=F32)
        res[:, g * LANES : (g + 1) * LANES] = picked.astype(BF16)

    for kind in kinds:
        loads[3 + kind].wait()
    if hz > 1:
        two_sides(hz - 1)
    far = lax.rem(me_z + hz, nz)

    def store_kind(layer, kind, value):
        if kind == 2:
            qbuf[...] = value.astype(BF16)
            return
        kv[layer, kind, toks : 2 * toks] = value.astype(BF16)
        src = kv.at[layer, kind, pl.ds(toks, toks)]
        for side in (0, 1):
            dst = kv.at[layer, kind, pl.ds(2 * toks if side == 0 else 0, toks)]
            send(src, dst, halo_send.at[layer], halo_recv.at[layer, kind, side], halo_dev[side])

    def finish_kind(kind):
        wait_bytes(w0.at[0, 0], part_sem(0, kind, hz))
        store_kind(0, kind, acc[:, kind * wide : (kind + 1) * wide] + qkv_block(far, kind))

    ring_hop(0, 0, hz)
    ring_hop(0, 1, hz)
    finish_kind(0)
    ring_hop(0, 2, hz)
    finish_kind(1)
    run_slot(hz)
    finish_kind(2)

    q_col = lax.broadcasted_iota(jnp.int32, (GRID_W, KR * GRID_W), 0)
    k_col = lax.broadcasted_iota(jnp.int32, (GRID_W, KR * GRID_W), 1) % GRID_W
    first_col = jnp.clip(q_col - KC // 2, 0, GRID_W - KC)
    inside = (k_col >= first_col) & (k_col < first_col + KC)
    grid_rows = rows * nsp

    def span(i):
        start = jnp.clip(me_s * rows + i - KR // 2, 0, grid_rows - KR) - (me_s * rows - rows)
        return start, pl.ds(pl.multiple_of(start * GRID_W, GRID_W), KR * GRID_W)

    def weigh(layer, i, head):
        start, keys_at = span(i)
        lanes = slice(head * HD, (head + 1) * HD)
        q = qbuf[i * GRID_W : (i + 1) * GRID_W, lanes]
        scores = nt_dot(q, kv[layer, 0, keys_at, lanes]) * (HD**-0.5)
        offset = start - rows - i + KR - 1
        pairs = []
        for p in range(KR // 2):
            line = lines[layer, head, pl.ds(offset + 2 * p, 1), :]
            spread = jnp.broadcast_to(line, (GRID_W, LANES))
            pairs.append(pltpu.roll(spread, 0, 1, stride=1, stride_axis=0))
        scores = scores + jnp.concatenate(pairs, axis=1)
        scores = jnp.where(inside, scores, -jnp.inf)
        e = jnp.exp(scores - jnp.max(scores, axis=-1, keepdims=True))
        return (e / jnp.sum(e, axis=-1, keepdims=True)).astype(BF16)

    def mix(layer, i, head, weights):
        lanes = slice(head * HD, (head + 1) * HD)
        values = kv[layer, 1, span(i)[1], lanes]
        mixed = jnp.dot(weights, values, preferred_element_type=F32)
        att[layer, me_x, i, :, lanes] = mixed.astype(BF16)

    def att_hop(layer, i, hop):
        for side in (0, 1):
            last = reach(nx, i % 2)[side]
            if hop > last:
                continue
            src = att.at[layer, ring_x(-hop if side == 0 else hop), i]
            if hop > 0:
                wait_bytes(src, att_recv.at[i, side * hx + hop - 1])
            if hop < last:
                slot = att_recv.at[i, side * hx + hop]
                send(src, src, att_send.at[layer, side], slot, x_dev[side])

    def halo_wait(layer, kind):
        for side in (0, 1):
            dst = kv.at[layer, kind, pl.ds(2 * toks if side == 0 else 0, toks)]
            wait_bytes(dst, halo_recv.at[layer, kind, side])

    def attention(layer, counts, until):
        if layer == 0:
            service(1)
        halo_wait(layer, 0)
        for i in range(0, rows, 2):
            weights = [weigh(layer, i + n // 2, n % 2) for n in range(4)]
            if i == 0:
                halo_wait(layer, 1)
            for n in range(4):
                mix(layer, i + n // 2, n % 2, weights[n])
            att_hop(layer, i, 0)
            att_hop(layer, i + 1, 0)
            service(counts[i // 2])
        for hop in range(1, hx + 1):
            for i in range(rows):
                att_hop(layer, i, hop)
            service(counts[1 + hop] if 1 + hop < len(counts) else 0)
        service(len(slots), until)

    def x_hop(layer, h, hop):
        buf = xbuf if layer == 0 else ybuf
        for side in (0, 1):
            last = reach(nx, h)[side]
            if hop > last:
                continue
            owner = ring_x(-hop if side == 0 else hop)
            src = buf.at[owner, h]
            if hop > 0:
                wait_bytes(src, x_recv.at[h, side * hx + hop - 1])
            if hop < last:
                slot = x_recv.at[h, side * hx + hop]
                send(src, src, x_send.at[layer, side], slot, x_dev[side])
            if layer == 1 and (hop > 0 or side == 0):
                pltpu.make_async_copy(src, out.at[owner, h], out_sem).start()

    def project(layer):
        wait_bytes(wo.at[layer, pl.ds(0, nz)], part_recv.at[hz + 1 + layer])
        buf = xbuf if layer == 0 else ybuf
        for h in (0, 1):
            total = None
            for x in range(nx):
                a = att[layer, x, h * (rows // 2) : (h + 1) * (rows // 2)].reshape(half, wide)
                w = wo[layer, :, :, x * wide : (x + 1) * wide].reshape(piece_w, wide)
                term = nt_dot(a, w)
                total = term if total is None else total + term
            own = res[h * half : (h + 1) * half] if layer == 0 else xbuf[me_x, h]
            buf[me_x, h] = (own.astype(F32) + total).astype(BF16)
            x_hop(layer, h, 0)

    attention(0, (1, 1, 1, 1, 0, 0), hz + lag)
    project(0)

    ss[...] = jnp.zeros_like(ss)

    def take_piece(owner, h):
        def some_rows(i, carry):
            at = pl.ds(pl.multiple_of(i * block, block), block)
            to = pl.ds(pl.multiple_of(h * half + i * block, block), block)
            x = xbuf[owner, h, at].astype(F32)
            squares = x * x
            total = ss[to]
            for g in range(piece_w // LANES):
                total = total + squares[:, g * LANES : (g + 1) * LANES]
            ss[to] = total
            lanes = pl.ds(pl.multiple_of(owner * piece_w, piece_w), piece_w)
            xn[to, lanes] = (x * gain1[owner]).astype(BF16)
            return carry

        lax.fori_loop(0, half // block, some_rows, 0)

    for h in (0, 1):
        take_piece(me_x, h)
    for hop in range(1, hx + 1):
        for h in (0, 1):
            service(1, 2 * hz + lag)
            x_hop(0, h, hop)
            both = [ring_x(-hop), ring_x(hop)]
            for owner in both if hop < hx else both[:1]:
                take_piece(owner, h)
    service(len(slots), 2 * hz + lag)
    wait_bytes(w0.at[:, pl.ds(0, nz)], part_recv.at[hz + 3])
    mean = jnp.sum(ss[...], axis=-1, keepdims=True) * (1.0 / depth)
    scale = lax.rsqrt(mean + norm_eps)
    for kind in kinds:
        w = w1[kind].reshape(depth, wide)
        store_kind(1, kind, jnp.dot(xn[...], w, preferred_element_type=F32) * scale)
    attention(1, (1, 1, 1, 1, 0, 0), 2 * hz + 2 * lag)
    project(1)
    for hop in range(1, hx + 1):
        for h in (0, 1):
            x_hop(1, h, hop)

    wait_bytes(ybuf, out_sem)
    chunks = 4 * hz - 2
    for side in (0, 1):
        wait_bytes(w0.at[pl.ds(0, 2), pl.ds(0, chunks)], z_send.at[side])
        for layer in range(LAYERS):
            wait_bytes(att.at[0, pl.ds(0, 2 * hx - 1), pl.ds(0, 2)], att_send.at[layer, side])
            wait_bytes(xbuf.at[pl.ds(0, 2 * hx - 1), 0], x_send.at[layer, side])
    for layer in range(LAYERS):
        wait_bytes(w0.at[pl.ds(0, 2)], part_send.at[layer])
        wait_bytes(kv.at[layer, :, pl.ds(0, 2 * toks)], halo_send.at[layer])
    wait_bytes(wt.at[:, pl.ds(0, nx - 1)], a2a_send)


def reorder_kernel(nx, y, o):
    half = y.shape[2]
    block = 32

    def some_rows(i, carry):
        at = pl.ds(pl.multiple_of(i * block, block), block)
        for h in (0, 1):
            to = pl.ds(pl.multiple_of(h * half + i * block, block), block)
            tiles = exchange([y[x, h, at, :].astype(F32) for x in range(nx)])
            for x in range(nx):
                o[to, x * LANES : (x + 1) * LANES] = tiles[x].astype(BF16)
        return carry

    lax.fori_loop(0, half // block, some_rows, 0)


def on_device(tokens, norm_gain, w_query, w_key, w_value, w_out, offset_bias):
    nsp, nx = lax.axis_size("sp"), lax.axis_size("tp")
    nz = nsp // 2
    hz, hx = nz // 2, nx // 2
    toks, depth = tokens.shape
    part = LANES // nx
    piece_w = depth // nx
    wide = 2 * HD
    rows = toks // GRID_W
    half = toks // 2

    def split(w):
        return w.reshape(LAYERS, nx, part, wide)

    vmem = pl.BlockSpec(memory_space=pltpu.VMEM)
    hbm = pl.BlockSpec(memory_space=pl.ANY)
    dma = pltpu.SemaphoreType.DMA
    y = pl.pallas_call(
        functools.partial(layers_kernel, nsp, nx),
        out_shape=jax.ShapeDtypeStruct((nx, 2, half, piece_w), BF16),
        in_specs=[hbm, vmem, hbm, hbm, hbm, hbm, vmem],
        out_specs=hbm,
        scratch_shapes=[
            pltpu.VMEM((toks, depth), BF16),
            pltpu.VMEM((LAYERS, wide, LANES), BF16),
            pltpu.VMEM((3, nsp, nx, part, wide), BF16),
            pltpu.VMEM((3, nx, nsp, part, wide), BF16),
            pltpu.VMEM((LAYERS, nsp, part, nx * wide), BF16),
            pltpu.VMEM((LAYERS, nx, part, wide), BF16),
            pltpu.VMEM((toks, depth), BF16),
            pltpu.VMEM((toks, 3 * wide), F32),
            pltpu.VMEM((toks, piece_w), BF16),
            pltpu.VMEM((toks, wide), BF16),
            pltpu.VMEM((LAYERS, 2, 3 * toks, wide), BF16),
            pltpu.VMEM((LAYERS, nx, rows, GRID_W, wide), BF16),
            pltpu.VMEM((nx, 2, half, piece_w), BF16),
            pltpu.VMEM((nx, 2, half, piece_w), BF16),
            pltpu.VMEM((toks, LANES), F32),
            pltpu.VMEM((nx, 1, piece_w), F32),
            pltpu.VMEM((LAYERS, 2 * KR + 1, 2, LANES), F32),
            pltpu.VMEM((LAYERS, 2, 2 * KR, LANES), F32),
            dma((8,)),
            dma((LAYERS, 4, 2 * hz)),
            dma((hz + 6,)),
            dma((LAYERS, 2, 2)),
            dma((rows, 2 * hx)),
            dma((2, 2 * hx)),
            dma((LAYERS,)),
            dma((2,)),
            dma((LAYERS,)),
            dma((LAYERS,)),
            dma((LAYERS, 2)),
            dma((LAYERS, 2)),
            dma(()),
            dma(()),
        ],
        compiler_params=pltpu.CompilerParams(
            collective_id=0, has_side_effects=True, vmem_limit_bytes=60 * 1024 * 1024
        ),
    )(
        tokens,
        norm_gain,
        split(w_query),
        split(w_key),
        split(w_value),
        w_out,
        offset_bias.swapaxes(1, 2),
    )
    return pl.pallas_call(
        functools.partial(reorder_kernel, nx),
        grid=(piece_w // LANES,),
        out_shape=jax.ShapeDtypeStruct((toks, depth), BF16),
        in_specs=[pl.BlockSpec((nx, 2, half, LANES), lambda g: (0, 0, 0, g))],
        out_specs=pl.BlockSpec((toks, nx * LANES), lambda g: (0, g)),
    )(y)


def solution(mesh):
    return jax.shard_map(
        on_device,
        mesh=mesh,
        in_specs=(
            P(("grp", "sp"), None),
            P(),
            P(None, "sp", "tp"),
            P(None, "sp", "tp"),
            P(None, "sp", "tp"),
            P(None, "tp", "sp"),
            P(None, "tp", None, None),
        ),
        out_specs=P(("grp", "sp"), None),
        check_vma=False,
    )
```

```python
import functools

import jax
import jax.numpy as jnp
from jax import lax
from jax.experimental import pallas as pl
from jax.experimental.pallas import tpu as pltpu
from jax.sharding import PartitionSpec as P

HD = 128
GRID_W = 64
KR = 8
KC = 16
LAYERS = 2
LANES = 128
MESH = pl.DeviceIdType.MESH
F32 = jnp.float32
BF16 = jnp.bfloat16

norm_eps = 1e-06


def reach(n, parity):
    plus = n // 2 if parity == 0 else n // 2 - 1
    return plus, n - 1 - plus


def nt_dot(a, b):
    return lax.dot_general(a, b, (((1,), (1,)), ((), ())), preferred_element_type=F32)


def wait_bytes(ref, sem):
    pltpu.make_async_copy(ref, ref, sem).wait()


def send(src, dst, send_sem, recv_sem, device):
    pltpu.make_async_remote_copy(
        src_ref=src,
        dst_ref=dst,
        send_sem=send_sem,
        recv_sem=recv_sem,
        device_id=device,
        device_id_type=MESH,
    ).start()


def exchange(tiles):
    tiles, n = list(tiles), len(tiles)
    part = LANES // n
    group = lax.broadcasted_iota(jnp.int32, tiles[0].shape, 1) // part
    bit = 1
    while bit < n:
        low = (group & bit) == 0
        for x in range(n):
            if x & bit == 0:
                a, b = tiles[x], tiles[x | bit]
                tiles[x] = jnp.where(low, a, pltpu.roll(b, bit * part, 1))
                tiles[x | bit] = jnp.where(low, pltpu.roll(a, LANES - bit * part, 1), b)
        bit *= 2
    return tiles


def layers_kernel(
    nsp,
    nx,
    tok_hbm,
    gain,
    wq,
    wk,
    wv,
    wout_hbm,
    bias,
    out,
    tok,
    wout,
    w0,
    w1,
    wo,
    wt,
    xn,
    acc,
    res,
    qbuf,
    kv,
    att,
    xbuf,
    ybuf,
    ss,
    gain1,
    padded,
    lines,
    load_sem,
    ring_recv,
    part_recv,
    halo_recv,
    att_recv,
    x_recv,
    a2a_recv,
    z_send,
    part_send,
    halo_send,
    att_send,
    x_send,
    a2a_send,
    out_sem,
):
    nz = nsp // 2
    hz, hx = nz // 2, nx // 2
    me_s, me_x = lax.axis_index("sp"), lax.axis_index("tp")
    me_z, me_c = me_s // 2, me_s % 2
    toks, depth = tok.shape
    part = LANES // nx
    wide = 2 * HD
    piece_w = depth // nx
    rows = toks // GRID_W
    half = toks // 2

    def ring_s(step):
        return lax.rem(me_s + 2 * step + 2 * nsp, nsp)

    def ring_x(step):
        return lax.rem(me_x + step + nx, nx)

    z_dev = ({"sp": ring_s(1)}, {"sp": ring_s(-1)})
    x_dev = ({"tp": ring_x(1)}, {"tp": ring_x(-1)})
    partner = {"sp": me_s + 1 - 2 * me_c}
    halo_dev = (
        {"sp": lax.rem(me_s + nsp - 1, nsp)},
        {"sp": lax.rem(me_s + 1, nsp)},
    )

    mats = (wk, wv, wq)
    kinds = (0, 1, 2)
    OUT = 3
    parity = (0, 1, 0, 1)
    lag = max(hz // 4, 1)
    out_from = hz + max(3 * hz // 4, 1)

    loads = [pltpu.make_async_copy(mats[k].at[0], w0.at[k, me_s], load_sem.at[k]) for k in kinds]
    loads += [
        pltpu.make_async_copy(mats[k].at[1], w1.at[k, :, me_s], load_sem.at[3 + k]) for k in kinds
    ]
    loads.append(pltpu.make_async_copy(wout_hbm, wout, load_sem.at[6]))
    loads.append(pltpu.make_async_copy(tok_hbm, tok, load_sem.at[7]))
    for load in loads:
        load.start()

    barrier = pltpu.get_barrier_semaphore()
    peers = [*z_dev, *halo_dev] + [{"tp": ring_x(d)} for d in range(1, nx)]
    for peer in peers:
        pl.semaphore_signal(barrier, inc=1, device_id=peer, device_id_type=MESH)
    pl.semaphore_wait(barrier, len(peers))

    def chunk(layer, kind, s):
        if kind == OUT:
            return wo.at[layer, s]
        return w0.at[kind, s] if layer == 0 else w1.at[kind, :, s]

    def part_sem(layer, kind, hop):
        if kind == OUT:
            return part_recv.at[hz + 1 + layer]
        if layer == 1:
            return part_recv.at[hz + 3]
        if isinstance(hop, int) and hop == hz:
            return part_recv.at[(hz, hz + 4, hz + 5)[kind]]
        return part_recv.at[hop]

    def ring_slot(layer, kind, side, hop):
        return ring_recv.at[layer, kind, side * hz + hop - 1]

    def ring_start(layer, kind):
        dst = chunk(layer, kind, me_s)
        for side in (0, 1):
            if reach(nz, parity[kind])[side] >= 1:
                send(dst, dst, z_send.at[side], ring_slot(layer, kind, side, 1), z_dev[side])
        send(dst, dst, part_send.at[layer], part_sem(layer, kind, 0), partner)

    def ring_hop(layer, kind, hop):
        for side in (0, 1):
            last = reach(nz, parity[kind])[side]
            if isinstance(hop, int) and hop > last:
                continue
            src = chunk(layer, kind, ring_s(-hop if side == 0 else hop))
            wait_bytes(src, ring_slot(layer, kind, side, hop))

            def onward(src=src, side=side):
                send(src, src, z_send.at[side], ring_slot(layer, kind, side, hop + 1), z_dev[side])

            if isinstance(hop, int):
                if hop < last:
                    onward()
            else:
                pl.when(hop < last)(onward)
            send(src, src, part_send.at[layer], part_sem(layer, kind, hop), partner)

    offsets = {(0, OUT): lag, (1, 0): hz, (1, 1): hz, (1, 2): hz, (1, OUT): out_from}

    def run_slot(slot):
        for what, offset in offsets.items():
            if 1 <= slot - offset <= hz:
                ring_hop(*what, slot - offset)
        for what, offset in offsets.items():
            if slot == offset:
                ring_start(*what)

    slots = list(range(hz + 1, out_from + hz + 1))

    def service(count, until=None):
        for _ in range(min(count, len(slots))):
            if until is None or slots[0] <= until:
                run_slot(slots.pop(0))

    for kind in kinds:
        loads[kind].wait()
        ring_start(0, kind)

    loads[6].wait()
    eye = (
        lax.broadcasted_iota(jnp.int32, (LANES, LANES), 0)
        == lax.broadcasted_iota(jnp.int32, (LANES, LANES), 1)
    ).astype(BF16)
    for layer in range(LAYERS):
        turned = nt_dot(eye, wout[layer]).astype(BF16)
        wt[layer] = turned.reshape(nx, part, wide)
    own_lanes = pl.ds(pl.multiple_of(me_x * wide, wide), wide)
    for layer in range(LAYERS):
        for d in range(1, nx):
            to = ring_x(d)
            send(
                wt.at[layer, to],
                wo.at[layer, me_s, :, own_lanes],
                a2a_send,
                a2a_recv.at[layer],
                {"tp": to},
            )
        wo[layer, me_s, :, own_lanes] = wt[layer, me_x]
    loads[7].wait()
    block = 32

    def norm_rows(i, carry):
        at = pl.ds(pl.multiple_of(i * block, block), block)
        x = tok[at, :].astype(F32)
        scaled = x * lax.rsqrt(jnp.mean(x * x, axis=-1, keepdims=True) + norm_eps)
        xn[at, :] = (scaled * gain[0:1].astype(F32)).astype(BF16)
        return carry

    lax.fori_loop(0, toks // block, norm_rows, 0)

    for x, tile in enumerate(
        exchange(
            [
                jnp.concatenate(
                    [
                        gain[1:2, (g * nx + t) * LANES : (g * nx + t + 1) * LANES].astype(F32)
                        for g in range(piece_w // LANES)
                    ],
                    axis=0,
                )
                for t in range(nx)
            ]
        )
    ):
        for g in range(piece_w // LANES):
            gain1[x, :, g * LANES : (g + 1) * LANES] = tile[g : g + 1]
    padded[...] = jnp.zeros_like(padded)
    padded[:, : 2 * KR - 1, :, : 2 * KC - 1] = bias[...]
    for layer in range(LAYERS):
        for head in (0, 1):
            here = pltpu.roll(padded[layer, : 2 * KR, head, :], LANES + 1 - KC, 1)
            after = pltpu.roll(padded[layer, 1 : 2 * KR + 1, head, :], GRID_W + 1 - KC, 1)
            lines[layer, head] = here + after

    def qkv_block(z, kind):
        x = xn[:, pl.ds(pl.multiple_of(z * 2 * LANES, 2 * LANES), 2 * LANES)]
        w = w0[kind, pl.ds(2 * z, 2)].reshape(2 * LANES, wide)
        return jnp.dot(x, w, preferred_element_type=F32)

    wait_bytes(w0.at[0, pl.ds(0, 3)], part_recv.at[0])
    for kind in kinds:
        acc[:, kind * wide : (kind + 1) * wide] = qkv_block(me_z, kind)

    def two_sides(hop):
        wait_bytes(w0.at[:, pl.ds(0, 2)], part_recv.at[hop])
        before = lax.rem(me_z - hop + nz, nz)
        after = lax.rem(me_z + hop, nz)
        for kind in kinds:
            acc[:, kind * wide : (kind + 1) * wide] += qkv_block(before, kind) + qkv_block(
                after, kind
            )

    def ring_step(with_out, hop, carry):
        for kind in kinds:
            ring_hop(0, kind, hop)
        if with_out:
            ring_hop(0, OUT, hop - lag)

        @pl.when(hop > 1)
        def _():
            two_sides(hop - 1)

        return carry

    split_at = min(lag + 1, hz)
    lax.fori_loop(1, split_at, functools.partial(ring_step, False), 0)
    for layer in range(LAYERS):
        wait_bytes(wt.at[layer, pl.ds(0, nx - 1)], a2a_recv.at[layer])
    if lag < hz:
        ring_start(0, OUT)
    lax.fori_loop(split_at, hz, functools.partial(ring_step, True), 0)

    group = nx * LANES
    sel_row = lax.broadcasted_iota(jnp.int32, (group, LANES), 0)
    sel_col = lax.broadcasted_iota(jnp.int32, (group, LANES), 1)
    pick = (sel_col // part) * LANES + me_x * part + sel_col % part
    sel = (sel_row == pick).astype(BF16)
    for g in range(depth // group):
        picked = jnp.dot(tok[:, g * group : (g + 1) * group], sel, preferred_element_type=F32)
        res[:, g * LANES : (g + 1) * LANES] = picked.astype(BF16)

    for kind in kinds:
        loads[3 + kind].wait()
    if hz > 1:
        two_sides(hz - 1)
    far = lax.rem(me_z + hz, nz)

    def store_kind(layer, kind, value):
        if kind == 2:
            qbuf[...] = value.astype(BF16)
            return
        kv[layer, kind, toks : 2 * toks] = value.astype(BF16)
        src = kv.at[layer, kind, pl.ds(toks, toks)]
        for side in (0, 1):
            dst = kv.at[layer, kind, pl.ds(2 * toks if side == 0 else 0, toks)]
            send(src, dst, halo_send.at[layer], halo_recv.at[layer, kind, side], halo_dev[side])

    def finish_kind(kind):
        wait_bytes(w0.at[0, 0], part_sem(0, kind, hz))
        store_kind(0, kind, acc[:, kind * wide : (kind + 1) * wide] + qkv_block(far, kind))

    ring_hop(0, 0, hz)
    ring_hop(0, 1, hz)
    finish_kind(0)
    ring_hop(0, 2, hz)
    finish_kind(1)
    run_slot(hz)
    finish_kind(2)

    q_col = lax.broadcasted_iota(jnp.int32, (GRID_W, KR * GRID_W), 0)
    k_col = lax.broadcasted_iota(jnp.int32, (GRID_W, KR * GRID_W), 1) % GRID_W
    first_col = jnp.clip(q_col - KC // 2, 0, GRID_W - KC)
    inside = (k_col >= first_col) & (k_col < first_col + KC)
    grid_rows = rows * nsp

    def span(i):
        start = jnp.clip(me_s * rows + i - KR // 2, 0, grid_rows - KR) - (me_s * rows - rows)
        return start, pl.ds(pl.multiple_of(start * GRID_W, GRID_W), KR * GRID_W)

    def weigh(layer, i, head):
        start, keys_at = span(i)
        lanes = slice(head * HD, (head + 1) * HD)
        q = qbuf[i * GRID_W : (i + 1) * GRID_W, lanes]
        scores = nt_dot(q, kv[layer, 0, keys_at, lanes]) * (HD**-0.5)
        offset = start - rows - i + KR - 1
        pairs = []
        for p in range(KR // 2):
            line = lines[layer, head, pl.ds(offset + 2 * p, 1), :]
            spread = jnp.broadcast_to(line, (GRID_W, LANES))
            pairs.append(pltpu.roll(spread, 0, 1, stride=1, stride_axis=0))
        scores = scores + jnp.concatenate(pairs, axis=1)
        scores = jnp.where(inside, scores, -jnp.inf)
        e = jnp.exp(scores - jnp.max(scores, axis=-1, keepdims=True))
        return (e / jnp.sum(e, axis=-1, keepdims=True)).astype(BF16)

    def mix(layer, i, head, weights):
        lanes = slice(head * HD, (head + 1) * HD)
        values = kv[layer, 1, span(i)[1], lanes]
        mixed = jnp.dot(weights, values, preferred_element_type=F32)
        att[layer, me_x, i, :, lanes] = mixed.astype(BF16)

    def att_hop(layer, i, hop):
        for side in (0, 1):
            last = reach(nx, i % 2)[side]
            if hop > last:
                continue
            src = att.at[layer, ring_x(-hop if side == 0 else hop), i]
            if hop > 0:
                wait_bytes(src, att_recv.at[i, side * hx + hop - 1])
            if hop < last:
                slot = att_recv.at[i, side * hx + hop]
                send(src, src, att_send.at[layer, side], slot, x_dev[side])

    def halo_wait(layer, kind):
        for side in (0, 1):
            dst = kv.at[layer, kind, pl.ds(2 * toks if side == 0 else 0, toks)]
            wait_bytes(dst, halo_recv.at[layer, kind, side])

    def attention(layer, counts, until):
        halo_wait(layer, 0)
        for i in range(0, rows, 2):
            weights = [weigh(layer, i + n // 2, n % 2) for n in range(4)]
            if i == 0:
                halo_wait(layer, 1)
            for n in range(4):
                mix(layer, i + n // 2, n % 2, weights[n])
            att_hop(layer, i, 0)
            att_hop(layer, i + 1, 0)
            service(counts[i // 2])
        for hop in range(1, hx + 1):
            for i in range(rows):
                att_hop(layer, i, hop)
            service(counts[1 + hop] if 1 + hop < len(counts) else 0)
        service(len(slots), until)

    def x_hop(layer, h, hop):
        buf = xbuf if layer == 0 else ybuf
        for side in (0, 1):
            last = reach(nx, h)[side]
            if hop > last:
                continue
            owner = ring_x(-hop if side == 0 else hop)
            src = buf.at[owner, h]
            if hop > 0:
                wait_bytes(src, x_recv.at[h, side * hx + hop - 1])
            if hop < last:
                slot = x_recv.at[h, side * hx + hop]
                send(src, src, x_send.at[layer, side], slot, x_dev[side])
            if layer == 1 and (hop > 0 or side == 0):
                pltpu.make_async_copy(src, out.at[owner, h], out_sem).start()

    def project(layer):
        wait_bytes(wo.at[layer, pl.ds(0, nz)], part_recv.at[hz + 1 + layer])
        buf = xbuf if layer == 0 else ybuf
        for h in (0, 1):
            total = None
            for x in range(nx):
                a = att[layer, x, h * (rows // 2) : (h + 1) * (rows // 2)].reshape(half, wide)
                w = wo[layer, :, :, x * wide : (x + 1) * wide].reshape(piece_w, wide)
                term = nt_dot(a, w)
                total = term if total is None else total + term
            own = res[h * half : (h + 1) * half] if layer == 0 else xbuf[me_x, h]
            buf[me_x, h] = (own.astype(F32) + total).astype(BF16)
            x_hop(layer, h, 0)

    attention(0, (1, 0, 1, 0, 1, 0), hz + lag)
    project(0)

    ss[...] = jnp.zeros_like(ss)

    def take_piece(owner, h):
        def some_rows(i, carry):
            at = pl.ds(pl.multiple_of(i * block, block), block)
            to = pl.ds(pl.multiple_of(h * half + i * block, block), block)
            x = xbuf[owner, h, at].astype(F32)
            squares = x * x
            total = ss[to]
            for g in range(piece_w // LANES):
                total = total + squares[:, g * LANES : (g + 1) * LANES]
            ss[to] = total
            lanes = pl.ds(pl.multiple_of(owner * piece_w, piece_w), piece_w)
            xn[to, lanes] = (x * gain1[owner]).astype(BF16)
            return carry

        lax.fori_loop(0, half // block, some_rows, 0)

    for h in (0, 1):
        take_piece(me_x, h)
    for hop in range(1, hx + 1):
        for h in (0, 1):
            if 2 * hop - 2 + h in (0, 1, 3, 5, 6):
                service(1, 2 * hz)
            x_hop(0, h, hop)
            both = [ring_x(-hop), ring_x(hop)]
            for owner in both if hop < hx else both[:1]:
                take_piece(owner, h)
    service(len(slots), 2 * hz)
    wait_bytes(w0.at[:, pl.ds(0, nz)], part_recv.at[hz + 3])
    mean = jnp.sum(ss[...], axis=-1, keepdims=True) * (1.0 / depth)
    scale = lax.rsqrt(mean + norm_eps)
    for kind in kinds:
        w = w1[kind].reshape(depth, wide)
        store_kind(1, kind, jnp.dot(xn[...], w, preferred_element_type=F32) * scale)
        service(1 if kind < 2 else 0)
    attention(1, (1, 1, 1, 1, 0, 0), out_from + hz)
    project(1)
    for hop in range(1, hx + 1):
        for h in (0, 1):
            x_hop(1, h, hop)

    wait_bytes(ybuf, out_sem)
    chunks = 4 * hz - 2
    for side in (0, 1):
        wait_bytes(w0.at[pl.ds(0, 2), pl.ds(0, chunks)], z_send.at[side])
        for layer in range(LAYERS):
            wait_bytes(att.at[0, pl.ds(0, 2 * hx - 1), pl.ds(0, 2)], att_send.at[layer, side])
            wait_bytes(xbuf.at[pl.ds(0, 2 * hx - 1), 0], x_send.at[layer, side])
    for layer in range(LAYERS):
        wait_bytes(w0.at[pl.ds(0, 2)], part_send.at[layer])
        wait_bytes(kv.at[layer, :, pl.ds(0, 2 * toks)], halo_send.at[layer])
    wait_bytes(wt.at[:, pl.ds(0, nx - 1)], a2a_send)


def reorder_kernel(nx, y, o):
    tiles = exchange([y[x].reshape(-1, LANES).astype(F32) for x in range(nx)])
    for x in range(nx):
        o[:, x * LANES : (x + 1) * LANES] = tiles[x].astype(BF16)


def on_device(tokens, norm_gain, w_query, w_key, w_value, w_out, offset_bias):
    nsp, nx = lax.axis_size("sp"), lax.axis_size("tp")
    nz = nsp // 2
    hz, hx = nz // 2, nx // 2
    toks, depth = tokens.shape
    part = LANES // nx
    piece_w = depth // nx
    wide = 2 * HD
    rows = toks // GRID_W
    half = toks // 2

    def split(w):
        return w.reshape(LAYERS, nx, part, wide)

    vmem = pl.BlockSpec(memory_space=pltpu.VMEM)
    hbm = pl.BlockSpec(memory_space=pl.ANY)
    dma = pltpu.SemaphoreType.DMA
    y = pl.pallas_call(
        functools.partial(layers_kernel, nsp, nx),
        out_shape=jax.ShapeDtypeStruct((nx, 2, half, piece_w), BF16),
        in_specs=[hbm, vmem, hbm, hbm, hbm, hbm, vmem],
        out_specs=hbm,
        scratch_shapes=[
            pltpu.VMEM((toks, depth), BF16),
            pltpu.VMEM((LAYERS, wide, LANES), BF16),
            pltpu.VMEM((3, nsp, nx, part, wide), BF16),
            pltpu.VMEM((3, nx, nsp, part, wide), BF16),
            pltpu.VMEM((LAYERS, nsp, part, nx * wide), BF16),
            pltpu.VMEM((LAYERS, nx, part, wide), BF16),
            pltpu.VMEM((toks, depth), BF16),
            pltpu.VMEM((toks, 3 * wide), F32),
            pltpu.VMEM((toks, piece_w), BF16),
            pltpu.VMEM((toks, wide), BF16),
            pltpu.VMEM((LAYERS, 2, 3 * toks, wide), BF16),
            pltpu.VMEM((LAYERS, nx, rows, GRID_W, wide), BF16),
            pltpu.VMEM((nx, 2, half, piece_w), BF16),
            pltpu.VMEM((nx, 2, half, piece_w), BF16),
            pltpu.VMEM((toks, LANES), F32),
            pltpu.VMEM((nx, 1, piece_w), F32),
            pltpu.VMEM((LAYERS, 2 * KR + 1, 2, LANES), F32),
            pltpu.VMEM((LAYERS, 2, 2 * KR, LANES), F32),
            dma((8,)),
            dma((LAYERS, 4, 2 * hz)),
            dma((hz + 6,)),
            dma((LAYERS, 2, 2)),
            dma((rows, 2 * hx)),
            dma((2, 2 * hx)),
            dma((LAYERS,)),
            dma((2,)),
            dma((LAYERS,)),
            dma((LAYERS,)),
            dma((LAYERS, 2)),
            dma((LAYERS, 2)),
            dma(()),
            dma(()),
        ],
        compiler_params=pltpu.CompilerParams(
            collective_id=0, has_side_effects=True, vmem_limit_bytes=60 * 1024 * 1024
        ),
    )(
        tokens,
        norm_gain,
        split(w_query),
        split(w_key),
        split(w_value),
        w_out,
        offset_bias.swapaxes(1, 2),
    )
    return pl.pallas_call(
        functools.partial(reorder_kernel, nx),
        grid=(piece_w // LANES,),
        out_shape=jax.ShapeDtypeStruct((toks, depth), BF16),
        in_specs=[pl.BlockSpec((nx, 2, half, LANES), lambda g: (0, 0, 0, g))],
        out_specs=pl.BlockSpec((toks, nx * LANES), lambda g: (0, g)),
    )(y)


def solution(mesh):
    return jax.shard_map(
        on_device,
        mesh=mesh,
        in_specs=(
            P(("grp", "sp"), None),
            P(),
            P(None, "sp", "tp"),
            P(None, "sp", "tp"),
            P(None, "sp", "tp"),
            P(None, "tp", "sp"),
            P(None, "tp", None, None),
        ),
        out_specs=P(("grp", "sp"), None),
        check_vma=False,
    )
```

```python
import functools

import jax
import jax.numpy as jnp
from jax import lax
from jax.experimental import pallas as pl
from jax.experimental.pallas import tpu as pltpu
from jax.sharding import PartitionSpec as P

HD = 128
GRID_W = 64
KR = 8
KC = 16
LAYERS = 2
LANES = 128
MESH = pl.DeviceIdType.MESH
F32 = jnp.float32
BF16 = jnp.bfloat16

norm_eps = 1e-06


def reach(n, parity):
    plus = n // 2 if parity == 0 else n // 2 - 1
    return plus, n - 1 - plus


def nt_dot(a, b):
    return lax.dot_general(a, b, (((1,), (1,)), ((), ())), preferred_element_type=F32)


def wait_bytes(ref, sem):
    pltpu.make_async_copy(ref, ref, sem).wait()


def send(src, dst, send_sem, recv_sem, device):
    pltpu.make_async_remote_copy(
        src_ref=src,
        dst_ref=dst,
        send_sem=send_sem,
        recv_sem=recv_sem,
        device_id=device,
        device_id_type=MESH,
    ).start()


def exchange(tiles):
    tiles, n = list(tiles), len(tiles)
    part = LANES // n
    group = lax.broadcasted_iota(jnp.int32, tiles[0].shape, 1) // part
    bit = 1
    while bit < n:
        low = (group & bit) == 0
        for x in range(n):
            if x & bit == 0:
                a, b = tiles[x], tiles[x | bit]
                tiles[x] = jnp.where(low, a, pltpu.roll(b, bit * part, 1))
                tiles[x | bit] = jnp.where(low, pltpu.roll(a, LANES - bit * part, 1), b)
        bit *= 2
    return tiles


def layers_kernel(
    nsp,
    nx,
    tok_hbm,
    gain,
    wq,
    wk,
    wv,
    wout_hbm,
    bias,
    out,
    tok,
    wout,
    w0,
    w1,
    wo,
    wt,
    xn,
    acc,
    res,
    qbuf,
    kv,
    att,
    xbuf,
    ybuf,
    ss,
    gain1,
    padded,
    lines,
    load_sem,
    ring_recv,
    part_recv,
    halo_recv,
    att_recv,
    x_recv,
    a2a_recv,
    z_send,
    part_send,
    halo_send,
    att_send,
    x_send,
    a2a_send,
    out_sem,
):
    nz = nsp // 2
    hz, hx = nz // 2, nx // 2
    me_s, me_x = lax.axis_index("sp"), lax.axis_index("tp")
    me_z, me_c = me_s // 2, me_s % 2
    toks, depth = tok.shape
    part = LANES // nx
    wide = 2 * HD
    piece_w = depth // nx
    rows = toks // GRID_W
    half = toks // 2

    def ring_s(step):
        return lax.rem(me_s + 2 * step + 2 * nsp, nsp)

    def ring_x(step):
        return lax.rem(me_x + step + nx, nx)

    z_dev = ({"sp": ring_s(1)}, {"sp": ring_s(-1)})
    x_dev = ({"tp": ring_x(1)}, {"tp": ring_x(-1)})
    partner = {"sp": me_s + 1 - 2 * me_c}
    halo_dev = (
        {"sp": lax.rem(me_s + nsp - 1, nsp)},
        {"sp": lax.rem(me_s + 1, nsp)},
    )

    mats = (wk, wv, wq)
    kinds = (0, 1, 2)
    OUT = 3
    parity = (0, 1, 0, 1, 1)
    lag = max(hz // 4, 1)
    out_from = hz + max(3 * hz // 4, 1)

    loads = [pltpu.make_async_copy(mats[k].at[0], w0.at[k, me_s], load_sem.at[k]) for k in kinds]
    loads += [
        pltpu.make_async_copy(mats[k].at[1], w1.at[k, :, me_s], load_sem.at[3 + k]) for k in kinds
    ]
    loads.append(pltpu.make_async_copy(wout_hbm, wout, load_sem.at[6]))
    loads.append(pltpu.make_async_copy(tok_hbm, tok, load_sem.at[7]))
    for load in loads:
        load.start()

    barrier = pltpu.get_barrier_semaphore()
    peers = [*z_dev, *halo_dev] + [{"tp": ring_x(d)} for d in range(1, nx)]
    for peer in peers:
        pl.semaphore_signal(barrier, inc=1, device_id=peer, device_id_type=MESH)
    pl.semaphore_wait(barrier, len(peers))

    def chunk(layer, kind, s):
        if kind >= OUT:
            lanes = nx * wide // (1 + layer)
            return wo.at[layer, s, :, pl.ds((kind - OUT) * lanes, lanes)]
        return w0.at[kind, s] if layer == 0 else w1.at[kind, :, s]

    def part_sem(layer, kind, hop):
        if kind >= OUT:
            return part_recv.at[hz + 1 + layer]
        if layer == 1:
            return part_recv.at[hz + 3]
        if isinstance(hop, int) and hop == hz:
            return part_recv.at[(hz, hz + 4, hz + 5)[kind]]
        return part_recv.at[hop]

    def ring_slot(layer, kind, side, hop):
        return ring_recv.at[4 * layer + kind, side * hz + hop - 1]

    def ring_start(layer, kind):
        dst = chunk(layer, kind, me_s)
        for side in (0, 1):
            if reach(nz, parity[kind])[side] >= 1:
                send(dst, dst, z_send.at[side], ring_slot(layer, kind, side, 1), z_dev[side])
        send(dst, dst, part_send.at[layer], part_sem(layer, kind, 0), partner)

    def ring_hop(layer, kind, hop):
        for side in (0, 1):
            last = reach(nz, parity[kind])[side]
            if isinstance(hop, int) and hop > last:
                continue
            src = chunk(layer, kind, ring_s(-hop if side == 0 else hop))
            wait_bytes(src, ring_slot(layer, kind, side, hop))

            def onward(src=src, side=side):
                send(src, src, z_send.at[side], ring_slot(layer, kind, side, hop + 1), z_dev[side])

            if isinstance(hop, int):
                if hop < last:
                    onward()
            else:
                pl.when(hop < last)(onward)
            send(src, src, part_send.at[layer], part_sem(layer, kind, hop), partner)

    offsets = {(0, OUT): lag, (1, 0): hz, (1, 1): hz, (1, 2): hz}
    offsets |= {(1, OUT): out_from, (1, OUT + 1): out_from}

    def run_slot(slot):
        for what, offset in offsets.items():
            if 1 <= slot - offset <= hz:
                ring_hop(*what, slot - offset)
        if slot != hz:
            start_after(slot)

    def start_after(slot):
        for what, offset in offsets.items():
            if slot == offset:
                ring_start(*what)

    slots = list(range(hz + 1, out_from + hz + 1))

    def service(count, until=None):
        for _ in range(min(count, len(slots))):
            if until is None or slots[0] <= until:
                run_slot(slots.pop(0))

    for kind in kinds:
        loads[kind].wait()
        ring_start(0, kind)

    loads[6].wait()
    eye = (
        lax.broadcasted_iota(jnp.int32, (LANES, LANES), 0)
        == lax.broadcasted_iota(jnp.int32, (LANES, LANES), 1)
    ).astype(BF16)
    for layer in range(LAYERS):
        turned = nt_dot(eye, wout[layer]).astype(BF16)
        wt[layer] = turned.reshape(nx, part, wide)
    own_lanes = pl.ds(pl.multiple_of(me_x * wide, wide), wide)
    for layer in range(LAYERS):
        for d in range(1, nx):
            to = ring_x(d)
            send(
                wt.at[layer, to],
                wo.at[layer, me_s, :, own_lanes],
                a2a_send,
                a2a_recv.at[layer],
                {"tp": to},
            )
        wo[layer, me_s, :, own_lanes] = wt[layer, me_x]
    loads[7].wait()
    block = 32

    def norm_rows(i, carry):
        at = pl.ds(pl.multiple_of(i * block, block), block)
        x = tok[at, :].astype(F32)
        scaled = x * lax.rsqrt(jnp.mean(x * x, axis=-1, keepdims=True) + norm_eps)
        xn[at, :] = (scaled * gain[0:1].astype(F32)).astype(BF16)
        return carry

    lax.fori_loop(0, toks // block, norm_rows, 0)

    for x, tile in enumerate(
        exchange(
            [
                jnp.concatenate(
                    [
                        gain[1:2, (g * nx + t) * LANES : (g * nx + t + 1) * LANES].astype(F32)
                        for g in range(piece_w // LANES)
                    ],
                    axis=0,
                )
                for t in range(nx)
            ]
        )
    ):
        for g in range(piece_w // LANES):
            gain1[x, :, g * LANES : (g + 1) * LANES] = tile[g : g + 1]
    padded[...] = jnp.zeros_like(padded)
    padded[:, : 2 * KR - 1, :, : 2 * KC - 1] = bias[...]
    for layer in range(LAYERS):
        for head in (0, 1):
            here = pltpu.roll(padded[layer, : 2 * KR, head, :], LANES + 1 - KC, 1)
            after = pltpu.roll(padded[layer, 1 : 2 * KR + 1, head, :], GRID_W + 1 - KC, 1)
            lines[layer, head] = here + after

    def qkv_block(z, kind):
        x = xn[:, pl.ds(pl.multiple_of(z * 2 * LANES, 2 * LANES), 2 * LANES)]
        w = w0[kind, pl.ds(2 * z, 2)].reshape(2 * LANES, wide)
        return jnp.dot(x, w, preferred_element_type=F32)

    wait_bytes(w0.at[0, pl.ds(0, 3)], part_recv.at[0])
    for kind in kinds:
        acc[:, kind * wide : (kind + 1) * wide] = qkv_block(me_z, kind)

    def two_sides(hop):
        wait_bytes(w0.at[:, pl.ds(0, 2)], part_recv.at[hop])
        before = lax.rem(me_z - hop + nz, nz)
        after = lax.rem(me_z + hop, nz)
        for kind in kinds:
            acc[:, kind * wide : (kind + 1) * wide] += qkv_block(before, kind) + qkv_block(
                after, kind
            )

    def ring_step(with_out, hop, carry):
        for kind in kinds:
            ring_hop(0, kind, hop)
        if with_out:
            ring_hop(0, OUT, hop - lag)

        @pl.when(hop > 1)
        def _():
            two_sides(hop - 1)

        return carry

    split_at = min(lag + 1, hz)
    lax.fori_loop(1, split_at, functools.partial(ring_step, False), 0)
    for layer in range(LAYERS):
        wait_bytes(wt.at[layer, pl.ds(0, nx - 1)], a2a_recv.at[layer])
    if lag < hz:
        ring_start(0, OUT)
    lax.fori_loop(split_at, hz, functools.partial(ring_step, True), 0)

    group = nx * LANES
    sel_row = lax.broadcasted_iota(jnp.int32, (group, LANES), 0)
    sel_col = lax.broadcasted_iota(jnp.int32, (group, LANES), 1)
    pick = (sel_col // part) * LANES + me_x * part + sel_col % part
    sel = (sel_row == pick).astype(BF16)
    for g in range(depth // group):
        picked = jnp.dot(tok[:, g * group : (g + 1) * group], sel, preferred_element_type=F32)
        res[:, g * LANES : (g + 1) * LANES] = picked.astype(BF16)

    for kind in kinds:
        loads[3 + kind].wait()
    if hz > 1:
        two_sides(hz - 1)
    far = lax.rem(me_z + hz, nz)

    def store_kind(layer, kind, value):
        if kind == 2:
            qbuf[...] = value.astype(BF16)
            return
        kv[layer, kind, toks : 2 * toks] = value.astype(BF16)
        src = kv.at[layer, kind, pl.ds(toks, toks)]
        for side in (0, 1):
            dst = kv.at[layer, kind, pl.ds(2 * toks if side == 0 else 0, toks)]
            send(src, dst, halo_send.at[layer], halo_recv.at[layer, kind, side], halo_dev[side])

    def finish_kind(kind):
        wait_bytes(w0.at[0, 0], part_sem(0, kind, hz))
        store_kind(0, kind, acc[:, kind * wide : (kind + 1) * wide] + qkv_block(far, kind))

    ring_hop(0, 0, hz)
    ring_hop(0, 1, hz)
    finish_kind(0)
    ring_hop(0, 2, hz)
    finish_kind(1)
    run_slot(hz)
    finish_kind(2)

    q_col = lax.broadcasted_iota(jnp.int32, (GRID_W, KR * GRID_W), 0)
    k_col = lax.broadcasted_iota(jnp.int32, (GRID_W, KR * GRID_W), 1) % GRID_W
    first_col = jnp.clip(q_col - KC // 2, 0, GRID_W - KC)
    inside = (k_col >= first_col) & (k_col < first_col + KC)
    grid_rows = rows * nsp

    def span(i):
        start = jnp.clip(me_s * rows + i - KR // 2, 0, grid_rows - KR) - (me_s * rows - rows)
        return start, pl.ds(pl.multiple_of(start * GRID_W, GRID_W), KR * GRID_W)

    def weigh(layer, i, head):
        start, keys_at = span(i)
        lanes = slice(head * HD, (head + 1) * HD)
        q = qbuf[i * GRID_W : (i + 1) * GRID_W, lanes]
        scores = nt_dot(q, kv[layer, 0, keys_at, lanes]) * (HD**-0.5)
        offset = start - rows - i + KR - 1
        pairs = []
        for p in range(KR // 2):
            line = lines[layer, head, pl.ds(offset + 2 * p, 1), :]
            spread = jnp.broadcast_to(line, (GRID_W, LANES))
            pairs.append(pltpu.roll(spread, 0, 1, stride=1, stride_axis=0))
        scores = scores + jnp.concatenate(pairs, axis=1)
        scores = jnp.where(inside, scores, -jnp.inf)
        e = jnp.exp(scores - jnp.max(scores, axis=-1, keepdims=True))
        return (e / jnp.sum(e, axis=-1, keepdims=True)).astype(BF16)

    def mix(layer, i, head, weights):
        lanes = slice(head * HD, (head + 1) * HD)
        values = kv[layer, 1, span(i)[1], lanes]
        mixed = jnp.dot(weights, values, preferred_element_type=F32)
        att[layer, me_x, i, :, lanes] = mixed.astype(BF16)

    def att_hop(layer, i, hop):
        for side in (0, 1):
            last = reach(nx, i % 2)[side]
            if hop > last:
                continue
            src = att.at[layer, ring_x(-hop if side == 0 else hop), i]
            if hop > 0:
                wait_bytes(src, att_recv.at[i, side * hx + hop - 1])
            if hop < last:
                slot = att_recv.at[i, side * hx + hop]
                send(src, src, att_send.at[layer, side], slot, x_dev[side])

    def halo_wait(layer, kind):
        for side in (0, 1):
            dst = kv.at[layer, kind, pl.ds(2 * toks if side == 0 else 0, toks)]
            wait_bytes(dst, halo_recv.at[layer, kind, side])

    def attention(layer, counts, until):
        halo_wait(layer, 0)
        if layer == 0:
            start_after(hz)
        for i in range(0, rows, 2):
            weights = [weigh(layer, i + n // 2, n % 2) for n in range(4)]
            if i == 0:
                halo_wait(layer, 1)
            for n in range(4):
                mix(layer, i + n // 2, n % 2, weights[n])
            att_hop(layer, i, 0)
            att_hop(layer, i + 1, 0)
            service(counts[i // 2])
        for hop in range(1, hx + 1):
            for i in range(rows):
                att_hop(layer, i, hop)
            service(counts[1 + hop] if 1 + hop < len(counts) else 0)
        service(len(slots), until)

    def x_hop(layer, h, hop):
        buf = xbuf if layer == 0 else ybuf
        for side in (0, 1):
            last = reach(nx, h)[side]
            if hop > last:
                continue
            owner = ring_x(-hop if side == 0 else hop)
            src = buf.at[owner, h]
            if hop > 0:
                wait_bytes(src, x_recv.at[h, side * hx + hop - 1])
            if hop < last:
                slot = x_recv.at[h, side * hx + hop]
                send(src, src, x_send.at[layer, side], slot, x_dev[side])
            if layer == 1 and (hop > 0 or side == 0):
                pltpu.make_async_copy(src, out.at[owner, h], out_sem).start()

    def project(layer):
        wait_bytes(wo.at[layer, pl.ds(0, nz)], part_recv.at[hz + 1 + layer])
        buf = xbuf if layer == 0 else ybuf
        for h in (0, 1):
            total = None
            for x in range(nx):
                a = att[layer, x, h * (rows // 2) : (h + 1) * (rows // 2)].reshape(half, wide)
                w = wo[layer, :, :, x * wide : (x + 1) * wide].reshape(piece_w, wide)
                term = nt_dot(a, w)
                total = term if total is None else total + term
            own = res[h * half : (h + 1) * half] if layer == 0 else xbuf[me_x, h]
            buf[me_x, h] = (own.astype(F32) + total).astype(BF16)
            x_hop(layer, h, 0)

    attention(0, (0, 1, 0, 1, 0, 1), hz + lag)
    project(0)

    ss[...] = jnp.zeros_like(ss)

    def take_piece(owner, h):
        def some_rows(i, carry):
            at = pl.ds(pl.multiple_of(i * block, block), block)
            to = pl.ds(pl.multiple_of(h * half + i * block, block), block)
            x = xbuf[owner, h, at].astype(F32)
            squares = x * x
            total = ss[to]
            for g in range(piece_w // LANES):
                total = total + squares[:, g * LANES : (g + 1) * LANES]
            ss[to] = total
            lanes = pl.ds(pl.multiple_of(owner * piece_w, piece_w), piece_w)
            xn[to, lanes] = (x * gain1[owner]).astype(BF16)
            return carry

        lax.fori_loop(0, half // block, some_rows, 0)

    for h in (0, 1):
        take_piece(me_x, h)
    for hop in range(1, hx + 1):
        for h in (0, 1):
            if 2 * hop - 2 + h in (0, 1, 3, 5, 6):
                service(1, 2 * hz)
            x_hop(0, h, hop)
            both = [ring_x(-hop), ring_x(hop)]
            for owner in both if hop < hx else both[:1]:
                take_piece(owner, h)
    service(len(slots), 2 * hz)
    wait_bytes(w0.at[:, pl.ds(0, nz)], part_recv.at[hz + 3])
    mean = jnp.sum(ss[...], axis=-1, keepdims=True) * (1.0 / depth)
    scale = lax.rsqrt(mean + norm_eps)
    for kind in kinds:
        w = w1[kind].reshape(depth, wide)
        store_kind(1, kind, jnp.dot(xn[...], w, preferred_element_type=F32) * scale)
        service(1 if kind == 1 else 0)
    attention(1, (1, 1, 1, 1, 1, 0), out_from + hz)
    project(1)
    for hop in range(1, hx + 1):
        for h in (0, 1):
            x_hop(1, h, hop)

    wait_bytes(ybuf, out_sem)
    chunks = 4 * hz - 2
    for side in (0, 1):
        wait_bytes(w0.at[pl.ds(0, 2), pl.ds(0, chunks)], z_send.at[side])
        for layer in range(LAYERS):
            wait_bytes(att.at[0, pl.ds(0, 2 * hx - 1), pl.ds(0, 2)], att_send.at[layer, side])
            wait_bytes(xbuf.at[pl.ds(0, 2 * hx - 1), 0], x_send.at[layer, side])
    for layer in range(LAYERS):
        wait_bytes(w0.at[pl.ds(0, 2)], part_send.at[layer])
        wait_bytes(kv.at[layer, :, pl.ds(0, 2 * toks)], halo_send.at[layer])
    wait_bytes(wt.at[:, pl.ds(0, nx - 1)], a2a_send)


def reorder_kernel(nx, y, o):
    tiles = exchange([y[x].reshape(-1, LANES).astype(F32) for x in range(nx)])
    for x in range(nx):
        o[:, x * LANES : (x + 1) * LANES] = tiles[x].astype(BF16)


def on_device(tokens, norm_gain, w_query, w_key, w_value, w_out, offset_bias):
    nsp, nx = lax.axis_size("sp"), lax.axis_size("tp")
    nz = nsp // 2
    hz, hx = nz // 2, nx // 2
    toks, depth = tokens.shape
    part = LANES // nx
    piece_w = depth // nx
    wide = 2 * HD
    rows = toks // GRID_W
    half = toks // 2

    def split(w):
        return w.reshape(LAYERS, nx, part, wide)

    vmem = pl.BlockSpec(memory_space=pltpu.VMEM)
    hbm = pl.BlockSpec(memory_space=pl.ANY)
    dma = pltpu.SemaphoreType.DMA
    y = pl.pallas_call(
        functools.partial(layers_kernel, nsp, nx),
        out_shape=jax.ShapeDtypeStruct((nx, 2, half, piece_w), BF16),
        in_specs=[hbm, vmem, hbm, hbm, hbm, hbm, vmem],
        out_specs=hbm,
        scratch_shapes=[
            pltpu.VMEM((toks, depth), BF16),
            pltpu.VMEM((LAYERS, wide, LANES), BF16),
            pltpu.VMEM((3, nsp, nx, part, wide), BF16),
            pltpu.VMEM((3, nx, nsp, part, wide), BF16),
            pltpu.VMEM((LAYERS, nsp, part, nx * wide), BF16),
            pltpu.VMEM((LAYERS, nx, part, wide), BF16),
            pltpu.VMEM((toks, depth), BF16),
            pltpu.VMEM((toks, 3 * wide), F32),
            pltpu.VMEM((toks, piece_w), BF16),
            pltpu.VMEM((toks, wide), BF16),
            pltpu.VMEM((LAYERS, 2, 3 * toks, wide), BF16),
            pltpu.VMEM((LAYERS, nx, rows, GRID_W, wide), BF16),
            pltpu.VMEM((nx, 2, half, piece_w), BF16),
            pltpu.VMEM((nx, 2, half, piece_w), BF16),
            pltpu.VMEM((toks, LANES), F32),
            pltpu.VMEM((nx, 1, piece_w), F32),
            pltpu.VMEM((LAYERS, 2 * KR + 1, 2, LANES), F32),
            pltpu.VMEM((LAYERS, 2, 2 * KR, LANES), F32),
            dma((8,)),
            dma((9, 2 * hz)),
            dma((hz + 6,)),
            dma((LAYERS, 2, 2)),
            dma((rows, 2 * hx)),
            dma((2, 2 * hx)),
            dma((LAYERS,)),
            dma((2,)),
            dma((LAYERS,)),
            dma((LAYERS,)),
            dma((LAYERS, 2)),
            dma((LAYERS, 2)),
            dma(()),
            dma(()),
        ],
        compiler_params=pltpu.CompilerParams(
            collective_id=0, has_side_effects=True, vmem_limit_bytes=60 * 1024 * 1024
        ),
    )(
        tokens,
        norm_gain,
        split(w_query),
        split(w_key),
        split(w_value),
        w_out,
        offset_bias.swapaxes(1, 2),
    )
    return pl.pallas_call(
        functools.partial(reorder_kernel, nx),
        grid=(piece_w // LANES,),
        out_shape=jax.ShapeDtypeStruct((toks, depth), BF16),
        in_specs=[pl.BlockSpec((nx, 2, half, LANES), lambda g: (0, 0, 0, g))],
        out_specs=pl.BlockSpec((toks, nx * LANES), lambda g: (0, g)),
    )(y)


def solution(mesh):
    return jax.shard_map(
        on_device,
        mesh=mesh,
        in_specs=(
            P(("grp", "sp"), None),
            P(),
            P(None, "sp", "tp"),
            P(None, "sp", "tp"),
            P(None, "sp", "tp"),
            P(None, "tp", "sp"),
            P(None, "tp", None, None),
        ),
        out_specs=P(("grp", "sp"), None),
        check_vma=False,
    )
```

```python
import functools

import jax
import jax.numpy as jnp
from jax import lax
from jax.experimental import pallas as pl
from jax.experimental.pallas import tpu as pltpu
from jax.sharding import PartitionSpec as P

HD = 128
GRID_W = 64
KR = 8
KC = 16
LAYERS = 2
LANES = 128
MESH = pl.DeviceIdType.MESH
F32 = jnp.float32
BF16 = jnp.bfloat16

norm_eps = 1e-06


def reach(n, parity):
    plus = n // 2 if parity == 0 else n // 2 - 1
    return plus, n - 1 - plus


def nt_dot(a, b):
    return lax.dot_general(a, b, (((1,), (1,)), ((), ())), preferred_element_type=F32)


def wait_bytes(ref, sem):
    pltpu.make_async_copy(ref, ref, sem).wait()


def send(src, dst, send_sem, recv_sem, device):
    pltpu.make_async_remote_copy(
        src_ref=src,
        dst_ref=dst,
        send_sem=send_sem,
        recv_sem=recv_sem,
        device_id=device,
        device_id_type=MESH,
    ).start()


def exchange(tiles):
    tiles, n = list(tiles), len(tiles)
    part = LANES // n
    group = lax.broadcasted_iota(jnp.int32, tiles[0].shape, 1) // part
    bit = 1
    while bit < n:
        low = (group & bit) == 0
        for x in range(n):
            if x & bit == 0:
                a, b = tiles[x], tiles[x | bit]
                tiles[x] = jnp.where(low, a, pltpu.roll(b, bit * part, 1))
                tiles[x | bit] = jnp.where(low, pltpu.roll(a, LANES - bit * part, 1), b)
        bit *= 2
    return tiles


def layers_kernel(
    nsp,
    nx,
    tok_hbm,
    gain,
    wq,
    wk,
    wv,
    wout_hbm,
    bias,
    out,
    tok,
    wout,
    w0,
    w1,
    wo,
    wt,
    xn,
    acc,
    res,
    qbuf,
    kv,
    att,
    xbuf,
    ybuf,
    ss,
    gain1,
    padded,
    lines,
    load_sem,
    ring_recv,
    part_recv,
    halo_recv,
    att_recv,
    x_recv,
    a2a_recv,
    z_send,
    part_send,
    halo_send,
    att_send,
    x_send,
    a2a_send,
    out_sem,
):
    nz = nsp // 2
    hz, hx = nz // 2, nx // 2
    me_s, me_x = lax.axis_index("sp"), lax.axis_index("tp")
    me_z, me_c = me_s // 2, me_s % 2
    toks, depth = tok.shape
    part = LANES // nx
    wide = 2 * HD
    piece_w = depth // nx
    rows = toks // GRID_W
    half = toks // 2

    def ring_s(step):
        return lax.rem(me_s + 2 * step + 2 * nsp, nsp)

    def ring_x(step):
        return lax.rem(me_x + step + nx, nx)

    z_dev = ({"sp": ring_s(1)}, {"sp": ring_s(-1)})
    x_dev = ({"tp": ring_x(1)}, {"tp": ring_x(-1)})
    partner = {"sp": me_s + 1 - 2 * me_c}
    halo_dev = (
        {"sp": lax.rem(me_s + nsp - 1, nsp)},
        {"sp": lax.rem(me_s + 1, nsp)},
    )

    mats = (wk, wv, wq)
    kinds = (0, 1, 2)
    OUT = 3
    parity = (0, 1, 0, 1, 1)
    lag = max(hz // 4, 1)
    out_from = hz + max(3 * hz // 4, 1)

    loads = [pltpu.make_async_copy(mats[k].at[0], w0.at[k, me_s], load_sem.at[k]) for k in kinds]
    loads += [
        pltpu.make_async_copy(mats[k].at[1], w1.at[k, :, me_s], load_sem.at[3 + k]) for k in kinds
    ]
    loads.append(pltpu.make_async_copy(wout_hbm, wout, load_sem.at[6]))
    loads.append(pltpu.make_async_copy(tok_hbm, tok, load_sem.at[7]))
    for load in loads:
        load.start()

    barrier = pltpu.get_barrier_semaphore()
    peers = [*z_dev, *halo_dev] + [{"tp": ring_x(d)} for d in range(1, nx)]
    for peer in peers:
        pl.semaphore_signal(barrier, inc=1, device_id=peer, device_id_type=MESH)
    pl.semaphore_wait(barrier, len(peers))

    def chunk(layer, kind, s):
        if kind >= OUT:
            lanes = nx * wide // (1 + layer)
            return wo.at[layer, s, :, pl.ds((kind - OUT) * lanes, lanes)]
        return w0.at[kind, s] if layer == 0 else w1.at[kind, :, s]

    def part_sem(layer, kind, hop):
        if kind >= OUT:
            return part_recv.at[hz + 1 + layer]
        if layer == 1:
            return part_recv.at[hz + 3]
        if isinstance(hop, int) and hop == hz:
            return part_recv.at[(hz, hz + 4, hz + 5)[kind]]
        return part_recv.at[hop]

    def ring_slot(layer, kind, side, hop):
        return ring_recv.at[4 * layer + kind, side * hz + hop - 1]

    def ring_start(layer, kind):
        dst = chunk(layer, kind, me_s)
        for side in (0, 1):
            if reach(nz, parity[kind])[side] >= 1:
                send(dst, dst, z_send.at[side], ring_slot(layer, kind, side, 1), z_dev[side])
        send(dst, dst, part_send.at[layer], part_sem(layer, kind, 0), partner)

    def ring_hop(layer, kind, hop):
        for side in (0, 1):
            last = reach(nz, parity[kind])[side]
            if isinstance(hop, int) and hop > last:
                continue
            src = chunk(layer, kind, ring_s(-hop if side == 0 else hop))
            wait_bytes(src, ring_slot(layer, kind, side, hop))

            def onward(src=src, side=side):
                send(src, src, z_send.at[side], ring_slot(layer, kind, side, hop + 1), z_dev[side])

            if isinstance(hop, int):
                if hop < last:
                    onward()
            else:
                pl.when(hop < last)(onward)
            send(src, src, part_send.at[layer], part_sem(layer, kind, hop), partner)

    offsets = {(0, OUT): lag, (1, 0): hz, (1, 1): hz, (1, 2): hz}
    offsets |= {(1, OUT): out_from, (1, OUT + 1): out_from}

    def run_slot(slot):
        for what, offset in offsets.items():
            if 1 <= slot - offset <= hz:
                ring_hop(*what, slot - offset)
        if slot != hz:
            start_after(slot)

    def start_after(slot):
        for what, offset in offsets.items():
            if slot == offset:
                ring_start(*what)

    slots = list(range(hz + 1, out_from + hz + 1))

    def service(count, until=None):
        for _ in range(min(count, len(slots))):
            if until is None or slots[0] <= until:
                run_slot(slots.pop(0))

    for kind in kinds:
        loads[kind].wait()
        ring_start(0, kind)

    loads[6].wait()
    eye = (
        lax.broadcasted_iota(jnp.int32, (LANES, LANES), 0)
        == lax.broadcasted_iota(jnp.int32, (LANES, LANES), 1)
    ).astype(BF16)
    for layer in range(LAYERS):
        turned = nt_dot(eye, wout[layer]).astype(BF16)
        wt[layer] = turned.reshape(nx, part, wide)
    own_lanes = pl.ds(pl.multiple_of(me_x * wide, wide), wide)
    for layer in range(LAYERS):
        for d in range(1, nx):
            to = ring_x(d)
            send(
                wt.at[layer, to],
                wo.at[layer, me_s, :, own_lanes],
                a2a_send,
                a2a_recv.at[layer],
                {"tp": to},
            )
        wo[layer, me_s, :, own_lanes] = wt[layer, me_x]
    loads[7].wait()
    block = 32

    def norm_rows(i, carry):
        at = pl.ds(pl.multiple_of(i * block, block), block)
        x = tok[at, :].astype(F32)
        scaled = x * lax.rsqrt(jnp.mean(x * x, axis=-1, keepdims=True) + norm_eps)
        xn[at, :] = (scaled * gain[0:1].astype(F32)).astype(BF16)
        return carry

    lax.fori_loop(0, toks // block, norm_rows, 0)

    for x, tile in enumerate(
        exchange(
            [
                jnp.concatenate(
                    [
                        gain[1:2, (g * nx + t) * LANES : (g * nx + t + 1) * LANES].astype(F32)
                        for g in range(piece_w // LANES)
                    ],
                    axis=0,
                )
                for t in range(nx)
            ]
        )
    ):
        for g in range(piece_w // LANES):
            gain1[x, :, g * LANES : (g + 1) * LANES] = tile[g : g + 1]
    padded[...] = jnp.zeros_like(padded)
    padded[:, : 2 * KR - 1, :, : 2 * KC - 1] = bias[...]
    for layer in range(LAYERS):
        for head in (0, 1):
            here = pltpu.roll(padded[layer, : 2 * KR, head, :], LANES + 1 - KC, 1)
            after = pltpu.roll(padded[layer, 1 : 2 * KR + 1, head, :], GRID_W + 1 - KC, 1)
            lines[layer, head] = here + after

    def qkv_block(z, kind):
        x = xn[:, pl.ds(pl.multiple_of(z * 2 * LANES, 2 * LANES), 2 * LANES)]
        w = w0[kind, pl.ds(2 * z, 2)].reshape(2 * LANES, wide)
        return jnp.dot(x, w, preferred_element_type=F32)

    wait_bytes(w0.at[0, pl.ds(0, 3)], part_recv.at[0])
    for kind in kinds:
        acc[:, kind * wide : (kind + 1) * wide] = qkv_block(me_z, kind)

    def two_sides(hop):
        wait_bytes(w0.at[:, pl.ds(0, 2)], part_recv.at[hop])
        before = lax.rem(me_z - hop + nz, nz)
        after = lax.rem(me_z + hop, nz)
        for kind in kinds:
            acc[:, kind * wide : (kind + 1) * wide] += qkv_block(before, kind) + qkv_block(
                after, kind
            )

    def ring_step(with_out, hop, carry):
        for kind in kinds:
            ring_hop(0, kind, hop)
        if with_out:
            ring_hop(0, OUT, hop - lag)

        @pl.when(hop > 1)
        def _():
            two_sides(hop - 1)

        return carry

    split_at = min(lag + 1, hz)
    lax.fori_loop(1, split_at, functools.partial(ring_step, False), 0)
    for layer in range(LAYERS):
        wait_bytes(wt.at[layer, pl.ds(0, nx - 1)], a2a_recv.at[layer])
    if lag < hz:
        ring_start(0, OUT)
    lax.fori_loop(split_at, hz, functools.partial(ring_step, True), 0)

    group = nx * LANES
    sel_row = lax.broadcasted_iota(jnp.int32, (group, LANES), 0)
    sel_col = lax.broadcasted_iota(jnp.int32, (group, LANES), 1)
    pick = (sel_col // part) * LANES + me_x * part + sel_col % part
    sel = (sel_row == pick).astype(BF16)
    for g in range(depth // group):
        picked = jnp.dot(tok[:, g * group : (g + 1) * group], sel, preferred_element_type=F32)
        res[:, g * LANES : (g + 1) * LANES] = picked.astype(BF16)

    for kind in kinds:
        loads[3 + kind].wait()
    if hz > 1:
        two_sides(hz - 1)
    far = lax.rem(me_z + hz, nz)

    def store_kind(layer, kind, value):
        if kind == 2:
            qbuf[...] = value.astype(BF16)
            return
        kv[layer, kind, toks : 2 * toks] = value.astype(BF16)
        src = kv.at[layer, kind, pl.ds(toks, toks)]
        for side in (0, 1):
            dst = kv.at[layer, kind, pl.ds(2 * toks if side == 0 else 0, toks)]
            send(src, dst, halo_send.at[layer], halo_recv.at[layer, kind, side], halo_dev[side])

    def finish_kind(kind):
        wait_bytes(w0.at[0, 0], part_sem(0, kind, hz))
        store_kind(0, kind, acc[:, kind * wide : (kind + 1) * wide] + qkv_block(far, kind))

    ring_hop(0, 0, hz)
    ring_hop(0, 1, hz)
    finish_kind(0)
    ring_hop(0, 2, hz)
    finish_kind(1)
    run_slot(hz)
    finish_kind(2)

    q_col = lax.broadcasted_iota(jnp.int32, (GRID_W, KR * GRID_W), 0)
    k_col = lax.broadcasted_iota(jnp.int32, (GRID_W, KR * GRID_W), 1) % GRID_W
    first_col = jnp.clip(q_col - KC // 2, 0, GRID_W - KC)
    inside = (k_col >= first_col) & (k_col < first_col + KC)
    grid_rows = rows * nsp

    def span(i):
        start = jnp.clip(me_s * rows + i - KR // 2, 0, grid_rows - KR) - (me_s * rows - rows)
        return start, pl.ds(pl.multiple_of(start * GRID_W, GRID_W), KR * GRID_W)

    def weigh(layer, i, head):
        start, keys_at = span(i)
        lanes = slice(head * HD, (head + 1) * HD)
        q = qbuf[i * GRID_W : (i + 1) * GRID_W, lanes]
        scores = nt_dot(q, kv[layer, 0, keys_at, lanes]) * (HD**-0.5)
        offset = start - rows - i + KR - 1
        pairs = []
        for p in range(KR // 2):
            line = lines[layer, head, pl.ds(offset + 2 * p, 1), :]
            spread = jnp.broadcast_to(line, (GRID_W, LANES))
            pairs.append(pltpu.roll(spread, 0, 1, stride=1, stride_axis=0))
        scores = scores + jnp.concatenate(pairs, axis=1)
        scores = jnp.where(inside, scores, -jnp.inf)
        e = jnp.exp(scores - jnp.max(scores, axis=-1, keepdims=True))
        return (e / jnp.sum(e, axis=-1, keepdims=True)).astype(BF16)

    def mix(layer, i, head, weights):
        lanes = slice(head * HD, (head + 1) * HD)
        values = kv[layer, 1, span(i)[1], lanes]
        mixed = jnp.dot(weights, values, preferred_element_type=F32)
        att[layer, me_x, i, :, lanes] = mixed.astype(BF16)

    def att_hop(layer, i, hop):
        for side in (0, 1):
            last = reach(nx, i % 2)[side]
            if hop > last:
                continue
            src = att.at[layer, ring_x(-hop if side == 0 else hop), i]
            if hop > 0:
                wait_bytes(src, att_recv.at[i, side * hx + hop - 1])
            if hop < last:
                slot = att_recv.at[i, side * hx + hop]
                send(src, src, att_send.at[layer, side], slot, x_dev[side])

    def halo_wait(layer, kind):
        for side in (0, 1):
            dst = kv.at[layer, kind, pl.ds(2 * toks if side == 0 else 0, toks)]
            wait_bytes(dst, halo_recv.at[layer, kind, side])

    def attention(layer, counts, until):
        halo_wait(layer, 0)
        if layer == 0:
            start_after(hz)
        for i in range(0, rows, 2):
            weights = [weigh(layer, i + n // 2, n % 2) for n in range(4)]
            if i == 0:
                halo_wait(layer, 1)
            for n in range(4):
                mix(layer, i + n // 2, n % 2, weights[n])
            att_hop(layer, i, 0)
            att_hop(layer, i + 1, 0)
            service(counts[i // 2])
        for hop in range(1, hx + 1):
            for i in range(rows):
                att_hop(layer, i, hop)
            service(counts[1 + hop] if 1 + hop < len(counts) else 0)
        service(len(slots), until)

    def x_hop(layer, h, hop):
        buf = xbuf if layer == 0 else ybuf
        for side in (0, 1):
            last = reach(nx, h)[side]
            if hop > last:
                continue
            owner = ring_x(-hop if side == 0 else hop)
            src = buf.at[owner, h]
            if hop > 0:
                wait_bytes(src, x_recv.at[h, side * hx + hop - 1])
            if hop < last:
                slot = x_recv.at[h, side * hx + hop]
                send(src, src, x_send.at[layer, side], slot, x_dev[side])
            if layer == 1 and (hop > 0 or side == 0):
                pltpu.make_async_copy(src, out.at[owner, h], out_sem).start()

    def project(layer):
        wait_bytes(wo.at[layer, pl.ds(0, nz)], part_recv.at[hz + 1 + layer])
        buf = xbuf if layer == 0 else ybuf
        for h in (0, 1):
            total = None
            for x in range(nx):
                a = att[layer, x, h * (rows // 2) : (h + 1) * (rows // 2)].reshape(half, wide)
                w = wo[layer, :, :, x * wide : (x + 1) * wide].reshape(piece_w, wide)
                term = nt_dot(a, w)
                total = term if total is None else total + term
            own = res[h * half : (h + 1) * half] if layer == 0 else xbuf[me_x, h]
            buf[me_x, h] = (own.astype(F32) + total).astype(BF16)
            x_hop(layer, h, 0)

    attention(0, (0, 0, 1, 0, 1, 0), hz + lag)
    project(0)

    ss[...] = jnp.zeros_like(ss)

    def take_piece(owner, h):
        def some_rows(i, carry):
            at = pl.ds(pl.multiple_of(i * block, block), block)
            to = pl.ds(pl.multiple_of(h * half + i * block, block), block)
            x = xbuf[owner, h, at].astype(F32)
            squares = x * x
            total = ss[to]
            for g in range(piece_w // LANES):
                total = total + squares[:, g * LANES : (g + 1) * LANES]
            ss[to] = total
            lanes = pl.ds(pl.multiple_of(owner * piece_w, piece_w), piece_w)
            xn[to, lanes] = (x * gain1[owner]).astype(BF16)
            return carry

        lax.fori_loop(0, half // block, some_rows, 0)

    for h in (0, 1):
        take_piece(me_x, h)
    for hop in range(1, hx + 1):
        for h in (0, 1):
            if 2 * hop - 2 + h in (0, 1, 2, 4, 5, 6):
                service(1, 2 * hz)
            x_hop(0, h, hop)
            both = [ring_x(-hop), ring_x(hop)]
            for owner in both if hop < hx else both[:1]:
                take_piece(owner, h)
    service(len(slots), 2 * hz)
    wait_bytes(w0.at[:, pl.ds(0, nz)], part_recv.at[hz + 3])
    mean = jnp.sum(ss[...], axis=-1, keepdims=True) * (1.0 / depth)
    scale = lax.rsqrt(mean + norm_eps)
    for kind in kinds:
        w = w1[kind].reshape(depth, wide)
        store_kind(1, kind, jnp.dot(xn[...], w, preferred_element_type=F32) * scale)
        service(1 if kind == 1 else 0)
    attention(1, (0, 1, 1, 1, 1, 1), out_from + hz)
    project(1)
    for hop in range(1, hx + 1):
        for h in (0, 1):
            x_hop(1, h, hop)

    wait_bytes(ybuf, out_sem)
    chunks = 4 * hz - 2
    for side in (0, 1):
        wait_bytes(w0.at[pl.ds(0, 2), pl.ds(0, chunks)], z_send.at[side])
        for layer in range(LAYERS):
            wait_bytes(att.at[0, pl.ds(0, 2 * hx - 1), pl.ds(0, 2)], att_send.at[layer, side])
            wait_bytes(xbuf.at[pl.ds(0, 2 * hx - 1), 0], x_send.at[layer, side])
    for layer in range(LAYERS):
        wait_bytes(w0.at[pl.ds(0, 2)], part_send.at[layer])
        wait_bytes(kv.at[layer, :, pl.ds(0, 2 * toks)], halo_send.at[layer])
    wait_bytes(wt.at[:, pl.ds(0, nx - 1)], a2a_send)


def reorder_kernel(nx, y, o):
    tiles = exchange([y[x].reshape(-1, LANES).astype(F32) for x in range(nx)])
    for x in range(nx):
        o[:, x * LANES : (x + 1) * LANES] = tiles[x].astype(BF16)


def on_device(tokens, norm_gain, w_query, w_key, w_value, w_out, offset_bias):
    nsp, nx = lax.axis_size("sp"), lax.axis_size("tp")
    nz = nsp // 2
    hz, hx = nz // 2, nx // 2
    toks, depth = tokens.shape
    part = LANES // nx
    piece_w = depth // nx
    wide = 2 * HD
    rows = toks // GRID_W
    half = toks // 2

    def split(w):
        return w.reshape(LAYERS, nx, part, wide)

    vmem = pl.BlockSpec(memory_space=pltpu.VMEM)
    hbm = pl.BlockSpec(memory_space=pl.ANY)
    dma = pltpu.SemaphoreType.DMA
    y = pl.pallas_call(
        functools.partial(layers_kernel, nsp, nx),
        out_shape=jax.ShapeDtypeStruct((nx, 2, half, piece_w), BF16),
        in_specs=[hbm, vmem, hbm, hbm, hbm, hbm, vmem],
        out_specs=hbm,
        scratch_shapes=[
            pltpu.VMEM((toks, depth), BF16),
            pltpu.VMEM((LAYERS, wide, LANES), BF16),
            pltpu.VMEM((3, nsp, nx, part, wide), BF16),
            pltpu.VMEM((3, nx, nsp, part, wide), BF16),
            pltpu.VMEM((LAYERS, nsp, part, nx * wide), BF16),
            pltpu.VMEM((LAYERS, nx, part, wide), BF16),
            pltpu.VMEM((toks, depth), BF16),
            pltpu.VMEM((toks, 3 * wide), F32),
            pltpu.VMEM((toks, piece_w), BF16),
            pltpu.VMEM((toks, wide), BF16),
            pltpu.VMEM((LAYERS, 2, 3 * toks, wide), BF16),
            pltpu.VMEM((LAYERS, nx, rows, GRID_W, wide), BF16),
            pltpu.VMEM((nx, 2, half, piece_w), BF16),
            pltpu.VMEM((nx, 2, half, piece_w), BF16),
            pltpu.VMEM((toks, LANES), F32),
            pltpu.VMEM((nx, 1, piece_w), F32),
            pltpu.VMEM((LAYERS, 2 * KR + 1, 2, LANES), F32),
            pltpu.VMEM((LAYERS, 2, 2 * KR, LANES), F32),
            dma((8,)),
            dma((9, 2 * hz)),
            dma((hz + 6,)),
            dma((LAYERS, 2, 2)),
            dma((rows, 2 * hx)),
            dma((2, 2 * hx)),
            dma((LAYERS,)),
            dma((2,)),
            dma((LAYERS,)),
            dma((LAYERS,)),
            dma((LAYERS, 2)),
            dma((LAYERS, 2)),
            dma(()),
            dma(()),
        ],
        compiler_params=pltpu.CompilerParams(
            collective_id=0, has_side_effects=True, vmem_limit_bytes=60 * 1024 * 1024
        ),
    )(
        tokens,
        norm_gain,
        split(w_query),
        split(w_key),
        split(w_value),
        w_out,
        offset_bias.swapaxes(1, 2),
    )
    return pl.pallas_call(
        functools.partial(reorder_kernel, nx),
        grid=(piece_w // LANES,),
        out_shape=jax.ShapeDtypeStruct((toks, depth), BF16),
        in_specs=[pl.BlockSpec((nx, 2, half, LANES), lambda g: (0, 0, 0, g))],
        out_specs=pl.BlockSpec((toks, nx * LANES), lambda g: (0, g)),
    )(y)


def solution(mesh):
    return jax.shard_map(
        on_device,
        mesh=mesh,
        in_specs=(
            P(("grp", "sp"), None),
            P(),
            P(None, "sp", "tp"),
            P(None, "sp", "tp"),
            P(None, "sp", "tp"),
            P(None, "tp", "sp"),
            P(None, "tp", None, None),
        ),
        out_specs=P(("grp", "sp"), None),
        check_vma=False,
    )
```

```python
import functools

import jax
import jax.numpy as jnp
from jax import lax
from jax.experimental import pallas as pl
from jax.experimental.pallas import tpu as pltpu
from jax.sharding import PartitionSpec as P

HD = 128
GRID_W = 64
KR = 8
KC = 16
LAYERS = 2
LANES = 128
MESH = pl.DeviceIdType.MESH
F32 = jnp.float32
BF16 = jnp.bfloat16

norm_eps = 1e-06


def reach(n, parity):
    plus = n // 2 if parity == 0 else n // 2 - 1
    return plus, n - 1 - plus


def nt_dot(a, b):
    return lax.dot_general(a, b, (((1,), (1,)), ((), ())), preferred_element_type=F32)


def wait_bytes(ref, sem):
    pltpu.make_async_copy(ref, ref, sem).wait()


def send(src, dst, send_sem, recv_sem, device):
    pltpu.make_async_remote_copy(
        src_ref=src,
        dst_ref=dst,
        send_sem=send_sem,
        recv_sem=recv_sem,
        device_id=device,
        device_id_type=MESH,
    ).start()


def exchange(tiles):
    tiles, n = list(tiles), len(tiles)
    part = LANES // n
    group = lax.broadcasted_iota(jnp.int32, tiles[0].shape, 1) // part
    bit = 1
    while bit < n:
        low = (group & bit) == 0
        for x in range(n):
            if x & bit == 0:
                a, b = tiles[x], tiles[x | bit]
                tiles[x] = jnp.where(low, a, pltpu.roll(b, bit * part, 1))
                tiles[x | bit] = jnp.where(low, pltpu.roll(a, LANES - bit * part, 1), b)
        bit *= 2
    return tiles


def layers_kernel(
    nsp,
    nx,
    tok_hbm,
    gain,
    wq,
    wk,
    wv,
    wout_hbm,
    bias,
    out,
    tok,
    wout,
    w0,
    w1,
    wo,
    wt,
    xn,
    acc,
    res,
    qbuf,
    kv,
    att,
    xbuf,
    ybuf,
    ss,
    gain1,
    padded,
    lines,
    load_sem,
    ring_recv,
    part_recv,
    halo_recv,
    att_recv,
    x_recv,
    a2a_recv,
    z_send,
    part_send,
    halo_send,
    att_send,
    x_send,
    a2a_send,
    out_sem,
):
    nz = nsp // 2
    hz, hx = nz // 2, nx // 2
    me_s, me_x = lax.axis_index("sp"), lax.axis_index("tp")
    me_z, me_c = me_s // 2, me_s % 2
    toks, depth = tok.shape
    part = LANES // nx
    wide = 2 * HD
    piece_w = depth // nx
    rows = toks // GRID_W
    half = toks // 2

    def ring_s(step):
        return lax.rem(me_s + 2 * step + 2 * nsp, nsp)

    def ring_x(step):
        return lax.rem(me_x + step + nx, nx)

    z_dev = ({"sp": ring_s(1)}, {"sp": ring_s(-1)})
    x_dev = ({"tp": ring_x(1)}, {"tp": ring_x(-1)})
    partner = {"sp": me_s + 1 - 2 * me_c}
    halo_dev = (
        {"sp": lax.rem(me_s + nsp - 1, nsp)},
        {"sp": lax.rem(me_s + 1, nsp)},
    )

    mats = (wk, wv, wq)
    kinds = (0, 1, 2)
    OUT = 3
    parity = (0, 1, 0, 1, 1)
    lag = max(hz // 4, 1)
    out_from = 2 * hz

    loads = [pltpu.make_async_copy(mats[k].at[0], w0.at[k, me_s], load_sem.at[k]) for k in kinds]
    loads += [
        pltpu.make_async_copy(mats[k].at[1], w1.at[k, :, me_s], load_sem.at[3 + k]) for k in kinds
    ]
    loads.append(pltpu.make_async_copy(wout_hbm, wout, load_sem.at[6]))
    loads.append(pltpu.make_async_copy(tok_hbm, tok, load_sem.at[7]))
    for load in loads:
        load.start()

    barrier = pltpu.get_barrier_semaphore()
    peers = [*z_dev, *halo_dev] + [{"tp": ring_x(d)} for d in range(1, nx)]
    for peer in peers:
        pl.semaphore_signal(barrier, inc=1, device_id=peer, device_id_type=MESH)
    pl.semaphore_wait(barrier, len(peers))

    def chunk(layer, kind, s):
        if kind >= OUT:
            lanes = nx * wide // (1 + layer)
            return wo.at[layer, s, :, pl.ds((kind - OUT) * lanes, lanes)]
        return w0.at[kind, s] if layer == 0 else w1.at[kind, :, s]

    def part_sem(layer, kind, hop):
        if kind >= OUT:
            return part_recv.at[hz + 1 + layer]
        if layer == 1:
            return part_recv.at[hz + 3]
        if isinstance(hop, int) and hop == hz:
            return part_recv.at[(hz, hz + 4, hz + 5)[kind]]
        return part_recv.at[hop]

    def ring_slot(layer, kind, side, hop):
        return ring_recv.at[4 * layer + kind, side * hz + hop - 1]

    def ring_start(layer, kind):
        dst = chunk(layer, kind, me_s)
        for side in (0, 1):
            if reach(nz, parity[kind])[side] >= 1:
                send(dst, dst, z_send.at[side], ring_slot(layer, kind, side, 1), z_dev[side])
        send(dst, dst, part_send.at[layer], part_sem(layer, kind, 0), partner)

    def ring_hop(layer, kind, hop):
        for side in (0, 1):
            last = reach(nz, parity[kind])[side]
            if isinstance(hop, int) and hop > last:
                continue
            src = chunk(layer, kind, ring_s(-hop if side == 0 else hop))
            wait_bytes(src, ring_slot(layer, kind, side, hop))

            def onward(src=src, side=side):
                send(src, src, z_send.at[side], ring_slot(layer, kind, side, hop + 1), z_dev[side])

            if isinstance(hop, int):
                if hop < last:
                    onward()
            else:
                pl.when(hop < last)(onward)
            send(src, src, part_send.at[layer], part_sem(layer, kind, hop), partner)

    offsets = {(0, OUT): lag, (1, 0): hz, (1, 1): hz, (1, 2): hz}
    offsets |= {(1, OUT): out_from, (1, OUT + 1): out_from}

    def run_slot(slot):
        for what, offset in offsets.items():
            if 1 <= slot - offset <= hz:
                ring_hop(*what, slot - offset)
        if slot != hz:
            start_after(slot)

    def start_after(slot):
        for what, offset in offsets.items():
            if slot == offset:
                ring_start(*what)

    slots = list(range(hz + 1, out_from + hz + 1))

    def service(count, until=None):
        for _ in range(min(count, len(slots))):
            if until is None or slots[0] <= until:
                run_slot(slots.pop(0))

    for kind in kinds:
        loads[kind].wait()
        ring_start(0, kind)

    loads[6].wait()
    eye = (
        lax.broadcasted_iota(jnp.int32, (LANES, LANES), 0)
        == lax.broadcasted_iota(jnp.int32, (LANES, LANES), 1)
    ).astype(BF16)
    for layer in range(LAYERS):
        turned = nt_dot(eye, wout[layer]).astype(BF16)
        wt[layer] = turned.reshape(nx, part, wide)
    own_lanes = pl.ds(pl.multiple_of(me_x * wide, wide), wide)
    for layer in range(LAYERS):
        for d in range(1, nx):
            to = ring_x(d)
            send(
                wt.at[layer, to],
                wo.at[layer, me_s, :, own_lanes],
                a2a_send,
                a2a_recv.at[layer],
                {"tp": to},
            )
        wo[layer, me_s, :, own_lanes] = wt[layer, me_x]
    loads[7].wait()
    block = 32

    def norm_rows(i, carry):
        at = pl.ds(pl.multiple_of(i * block, block), block)
        x = tok[at, :].astype(F32)
        scaled = x * lax.rsqrt(jnp.mean(x * x, axis=-1, keepdims=True) + norm_eps)
        xn[at, :] = (scaled * gain[0:1].astype(F32)).astype(BF16)
        return carry

    lax.fori_loop(0, toks // block, norm_rows, 0)

    for x, tile in enumerate(
        exchange(
            [
                jnp.concatenate(
                    [
                        gain[1:2, (g * nx + t) * LANES : (g * nx + t + 1) * LANES].astype(F32)
                        for g in range(piece_w // LANES)
                    ],
                    axis=0,
                )
                for t in range(nx)
            ]
        )
    ):
        for g in range(piece_w // LANES):
            gain1[x, :, g * LANES : (g + 1) * LANES] = tile[g : g + 1]
    padded[...] = jnp.zeros_like(padded)
    padded[:, : 2 * KR - 1, :, : 2 * KC - 1] = bias[...]
    for layer in range(LAYERS):
        for head in (0, 1):
            here = pltpu.roll(padded[layer, : 2 * KR, head, :], LANES + 1 - KC, 1)
            after = pltpu.roll(padded[layer, 1 : 2 * KR + 1, head, :], GRID_W + 1 - KC, 1)
            lines[layer, head] = here + after

    def qkv_block(z, kind):
        x = xn[:, pl.ds(pl.multiple_of(z * 2 * LANES, 2 * LANES), 2 * LANES)]
        w = w0[kind, pl.ds(2 * z, 2)].reshape(2 * LANES, wide)
        return jnp.dot(x, w, preferred_element_type=F32)

    wait_bytes(w0.at[0, pl.ds(0, 3)], part_recv.at[0])
    for kind in kinds:
        acc[:, kind * wide : (kind + 1) * wide] = qkv_block(me_z, kind)

    def two_sides(hop):
        wait_bytes(w0.at[:, pl.ds(0, 2)], part_recv.at[hop])
        before = lax.rem(me_z - hop + nz, nz)
        after = lax.rem(me_z + hop, nz)
        for kind in kinds:
            acc[:, kind * wide : (kind + 1) * wide] += qkv_block(before, kind) + qkv_block(
                after, kind
            )

    def ring_step(with_out, hop, carry):
        for kind in kinds:
            ring_hop(0, kind, hop)
        if with_out:
            ring_hop(0, OUT, hop - lag)

        @pl.when(hop > 1)
        def _():
            two_sides(hop - 1)

        return carry

    split_at = min(lag + 1, hz)
    lax.fori_loop(1, split_at, functools.partial(ring_step, False), 0)
    for layer in range(LAYERS):
        wait_bytes(wt.at[layer, pl.ds(0, nx - 1)], a2a_recv.at[layer])
    if lag < hz:
        ring_start(0, OUT)
    lax.fori_loop(split_at, hz, functools.partial(ring_step, True), 0)

    group = nx * LANES
    sel_row = lax.broadcasted_iota(jnp.int32, (group, LANES), 0)
    sel_col = lax.broadcasted_iota(jnp.int32, (group, LANES), 1)
    pick = (sel_col // part) * LANES + me_x * part + sel_col % part
    sel = (sel_row == pick).astype(BF16)
    for g in range(depth // group):
        picked = jnp.dot(tok[:, g * group : (g + 1) * group], sel, preferred_element_type=F32)
        res[:, g * LANES : (g + 1) * LANES] = picked.astype(BF16)

    for kind in kinds:
        loads[3 + kind].wait()
    if hz > 1:
        two_sides(hz - 1)
    far = lax.rem(me_z + hz, nz)

    def store_kind(layer, kind, value):
        if kind == 2:
            qbuf[...] = value.astype(BF16)
            return
        kv[layer, kind, toks : 2 * toks] = value.astype(BF16)
        src = kv.at[layer, kind, pl.ds(toks, toks)]
        for side in (0, 1):
            dst = kv.at[layer, kind, pl.ds(2 * toks if side == 0 else 0, toks)]
            send(src, dst, halo_send.at[layer], halo_recv.at[layer, kind, side], halo_dev[side])

    def finish_kind(kind):
        wait_bytes(w0.at[0, 0], part_sem(0, kind, hz))
        store_kind(0, kind, acc[:, kind * wide : (kind + 1) * wide] + qkv_block(far, kind))

    ring_hop(0, 0, hz)
    ring_hop(0, 1, hz)
    finish_kind(0)
    ring_hop(0, 2, hz)
    finish_kind(1)
    run_slot(hz)
    finish_kind(2)

    q_col = lax.broadcasted_iota(jnp.int32, (GRID_W, KR * GRID_W), 0)
    k_col = lax.broadcasted_iota(jnp.int32, (GRID_W, KR * GRID_W), 1) % GRID_W
    first_col = jnp.clip(q_col - KC // 2, 0, GRID_W - KC)
    inside = (k_col >= first_col) & (k_col < first_col + KC)
    grid_rows = rows * nsp

    def span(i):
        start = jnp.clip(me_s * rows + i - KR // 2, 0, grid_rows - KR) - (me_s * rows - rows)
        return start, pl.ds(pl.multiple_of(start * GRID_W, GRID_W), KR * GRID_W)

    def weigh(layer, i, head):
        start, keys_at = span(i)
        lanes = slice(head * HD, (head + 1) * HD)
        q = qbuf[i * GRID_W : (i + 1) * GRID_W, lanes]
        scores = nt_dot(q, kv[layer, 0, keys_at, lanes]) * (HD**-0.5)
        offset = start - rows - i + KR - 1
        pairs = []
        for p in range(KR // 2):
            line = lines[layer, head, pl.ds(offset + 2 * p, 1), :]
            spread = jnp.broadcast_to(line, (GRID_W, LANES))
            pairs.append(pltpu.roll(spread, 0, 1, stride=1, stride_axis=0))
        scores = scores + jnp.concatenate(pairs, axis=1)
        scores = jnp.where(inside, scores, -jnp.inf)
        e = jnp.exp(scores - jnp.max(scores, axis=-1, keepdims=True))
        return (e / jnp.sum(e, axis=-1, keepdims=True)).astype(BF16)

    def mix(layer, i, head, weights):
        lanes = slice(head * HD, (head + 1) * HD)
        values = kv[layer, 1, span(i)[1], lanes]
        mixed = jnp.dot(weights, values, preferred_element_type=F32)
        att[layer, me_x, i, :, lanes] = mixed.astype(BF16)

    def att_hop(layer, i, hop):
        for side in (0, 1):
            last = reach(nx, i % 2)[side]
            if hop > last:
                continue
            src = att.at[layer, ring_x(-hop if side == 0 else hop), i]
            if hop > 0:
                wait_bytes(src, att_recv.at[i, side * hx + hop - 1])
            if hop < last:
                slot = att_recv.at[i, side * hx + hop]
                send(src, src, att_send.at[layer, side], slot, x_dev[side])

    def halo_wait(layer, kind):
        for side in (0, 1):
            dst = kv.at[layer, kind, pl.ds(2 * toks if side == 0 else 0, toks)]
            wait_bytes(dst, halo_recv.at[layer, kind, side])

    def attention(layer, counts, until):
        halo_wait(layer, 0)
        if layer == 0:
            start_after(hz)
        for i in range(0, rows, 2):
            weights = [weigh(layer, i + n // 2, n % 2) for n in range(4)]
            if i == 0:
                halo_wait(layer, 1)
            for n in range(4):
                mix(layer, i + n // 2, n % 2, weights[n])
            att_hop(layer, i, 0)
            att_hop(layer, i + 1, 0)
            service(counts[i // 2])
        for hop in range(1, hx + 1):
            for i in range(rows):
                att_hop(layer, i, hop)
            service(counts[1 + hop] if 1 + hop < len(counts) else 0)
        service(len(slots), until)

    def x_hop(layer, h, hop):
        buf = xbuf if layer == 0 else ybuf
        for side in (0, 1):
            last = reach(nx, h)[side]
            if hop > last:
                continue
            owner = ring_x(-hop if side == 0 else hop)
            src = buf.at[owner, h]
            if hop > 0:
                wait_bytes(src, x_recv.at[h, side * hx + hop - 1])
            if hop < last:
                slot = x_recv.at[h, side * hx + hop]
                send(src, src, x_send.at[layer, side], slot, x_dev[side])
            if layer == 1 and (hop > 0 or side == 0):
                pltpu.make_async_copy(src, out.at[owner, h], out_sem).start()

    def project(layer):
        wait_bytes(wo.at[layer, pl.ds(0, nz)], part_recv.at[hz + 1 + layer])
        buf = xbuf if layer == 0 else ybuf
        for h in (0, 1):
            total = None
            for x in range(nx):
                a = att[layer, x, h * (rows // 2) : (h + 1) * (rows // 2)].reshape(half, wide)
                w = wo[layer, :, :, x * wide : (x + 1) * wide].reshape(piece_w, wide)
                term = nt_dot(a, w)
                total = term if total is None else total + term
            own = res[h * half : (h + 1) * half] if layer == 0 else xbuf[me_x, h]
            buf[me_x, h] = (own.astype(F32) + total).astype(BF16)
            x_hop(layer, h, 0)

    attention(0, (0, 0, 1, 0, 1, 0), hz + lag)
    project(0)

    ss[...] = jnp.zeros_like(ss)

    def take_piece(owner, h):
        def some_rows(i, carry):
            at = pl.ds(pl.multiple_of(i * block, block), block)
            to = pl.ds(pl.multiple_of(h * half + i * block, block), block)
            x = xbuf[owner, h, at].astype(F32)
            squares = x * x
            total = ss[to]
            for g in range(piece_w // LANES):
                total = total + squares[:, g * LANES : (g + 1) * LANES]
            ss[to] = total
            lanes = pl.ds(pl.multiple_of(owner * piece_w, piece_w), piece_w)
            xn[to, lanes] = (x * gain1[owner]).astype(BF16)
            return carry

        lax.fori_loop(0, half // block, some_rows, 0)

    for h in (0, 1):
        take_piece(me_x, h)
    for hop in range(1, hx + 1):
        for h in (0, 1):
            if 2 * hop - 2 + h in (0, 1, 2, 4, 5, 6):
                service(1, 2 * hz)
            x_hop(0, h, hop)
            both = [ring_x(-hop), ring_x(hop)]
            for owner in both if hop < hx else both[:1]:
                take_piece(owner, h)
    service(len(slots), 2 * hz)
    wait_bytes(w0.at[:, pl.ds(0, nz)], part_recv.at[hz + 3])
    mean = jnp.sum(ss[...], axis=-1, keepdims=True) * (1.0 / depth)
    scale = lax.rsqrt(mean + norm_eps)
    for kind in kinds:
        w = w1[kind].reshape(depth, wide)
        store_kind(1, kind, jnp.dot(xn[...], w, preferred_element_type=F32) * scale)
        service(1 if kind == 1 else 0)
    attention(1, (1, 1, 1, 1, 1, 1), out_from + hz)
    project(1)
    for hop in range(1, hx + 1):
        for h in (0, 1):
            x_hop(1, h, hop)

    wait_bytes(ybuf, out_sem)
    chunks = 4 * hz - 2
    for side in (0, 1):
        wait_bytes(w0.at[pl.ds(0, 2), pl.ds(0, chunks)], z_send.at[side])
        for layer in range(LAYERS):
            wait_bytes(att.at[0, pl.ds(0, 2 * hx - 1), pl.ds(0, 2)], att_send.at[layer, side])
            wait_bytes(xbuf.at[pl.ds(0, 2 * hx - 1), 0], x_send.at[layer, side])
    for layer in range(LAYERS):
        wait_bytes(w0.at[pl.ds(0, 2)], part_send.at[layer])
        wait_bytes(kv.at[layer, :, pl.ds(0, 2 * toks)], halo_send.at[layer])
    wait_bytes(wt.at[:, pl.ds(0, nx - 1)], a2a_send)


def reorder_kernel(nx, y, o):
    tiles = exchange([y[x].reshape(-1, LANES).astype(F32) for x in range(nx)])
    for x in range(nx):
        o[:, x * LANES : (x + 1) * LANES] = tiles[x].astype(BF16)


def on_device(tokens, norm_gain, w_query, w_key, w_value, w_out, offset_bias):
    nsp, nx = lax.axis_size("sp"), lax.axis_size("tp")
    nz = nsp // 2
    hz, hx = nz // 2, nx // 2
    toks, depth = tokens.shape
    part = LANES // nx
    piece_w = depth // nx
    wide = 2 * HD
    rows = toks // GRID_W
    half = toks // 2

    def split(w):
        return w.reshape(LAYERS, nx, part, wide)

    vmem = pl.BlockSpec(memory_space=pltpu.VMEM)
    hbm = pl.BlockSpec(memory_space=pl.ANY)
    dma = pltpu.SemaphoreType.DMA
    y = pl.pallas_call(
        functools.partial(layers_kernel, nsp, nx),
        out_shape=jax.ShapeDtypeStruct((nx, 2, half, piece_w), BF16),
        in_specs=[hbm, vmem, hbm, hbm, hbm, hbm, vmem],
        out_specs=hbm,
        scratch_shapes=[
            pltpu.VMEM((toks, depth), BF16),
            pltpu.VMEM((LAYERS, wide, LANES), BF16),
            pltpu.VMEM((3, nsp, nx, part, wide), BF16),
            pltpu.VMEM((3, nx, nsp, part, wide), BF16),
            pltpu.VMEM((LAYERS, nsp, part, nx * wide), BF16),
            pltpu.VMEM((LAYERS, nx, part, wide), BF16),
            pltpu.VMEM((toks, depth), BF16),
            pltpu.VMEM((toks, 3 * wide), F32),
            pltpu.VMEM((toks, piece_w), BF16),
            pltpu.VMEM((toks, wide), BF16),
            pltpu.VMEM((LAYERS, 2, 3 * toks, wide), BF16),
            pltpu.VMEM((LAYERS, nx, rows, GRID_W, wide), BF16),
            pltpu.VMEM((nx, 2, half, piece_w), BF16),
            pltpu.VMEM((nx, 2, half, piece_w), BF16),
            pltpu.VMEM((toks, LANES), F32),
            pltpu.VMEM((nx, 1, piece_w), F32),
            pltpu.VMEM((LAYERS, 2 * KR + 1, 2, LANES), F32),
            pltpu.VMEM((LAYERS, 2, 2 * KR, LANES), F32),
            dma((8,)),
            dma((9, 2 * hz)),
            dma((hz + 6,)),
            dma((LAYERS, 2, 2)),
            dma((rows, 2 * hx)),
            dma((2, 2 * hx)),
            dma((LAYERS,)),
            dma((2,)),
            dma((LAYERS,)),
            dma((LAYERS,)),
            dma((LAYERS, 2)),
            dma((LAYERS, 2)),
            dma(()),
            dma(()),
        ],
        compiler_params=pltpu.CompilerParams(
            collective_id=0, has_side_effects=True, vmem_limit_bytes=60 * 1024 * 1024
        ),
    )(
        tokens,
        norm_gain,
        split(w_query),
        split(w_key),
        split(w_value),
        w_out,
        offset_bias.swapaxes(1, 2),
    )
    return pl.pallas_call(
        functools.partial(reorder_kernel, nx),
        grid=(piece_w // LANES,),
        out_shape=jax.ShapeDtypeStruct((toks, depth), BF16),
        in_specs=[pl.BlockSpec((nx, 2, half, LANES), lambda g: (0, 0, 0, g))],
        out_specs=pl.BlockSpec((toks, nx * LANES), lambda g: (0, g)),
    )(y)


def solution(mesh):
    return jax.shard_map(
        on_device,
        mesh=mesh,
        in_specs=(
            P(("grp", "sp"), None),
            P(),
            P(None, "sp", "tp"),
            P(None, "sp", "tp"),
            P(None, "sp", "tp"),
            P(None, "tp", "sp"),
            P(None, "tp", None, None),
        ),
        out_specs=P(("grp", "sp"), None),
        check_vma=False,
    )
```
